512 devices in a mesh: sp: 32 (over z, x), tp: 16 (over y, core).
Axes of the slice: x: 4, y: 8, z: 8, core: 2. Of those that a mesh axis runs over, the one named last changes fastest.
Arguments:
- queries: bfloat16 [8192, 1024], P('sp', 'tp'), may hold values from -6 to 6
- keys: bfloat16 [8192, 256], P('sp'), may hold values from -6 to 6
- values: bfloat16 [8192, 256], P('sp'), may hold values from -6 to 6
- sink: float32 [16], P('tp'), may hold values from 3 to 6
- w_out: bfloat16 [1024, 2048], P('tp'), may hold values from -0.1875 to 0.1875
- stream: bfloat16 [8192, 2048], P(('sp', 'tp')), may hold values from -6 to 6
- gain: bfloat16 [2048], replicated, may hold values from 0.099609375 to 1.8984375
- routes: int32 [8192, 4], P('sp'), may hold values from 0 to 63, all different within a row; in each aligned block of 16 rows (0 to 15, 16 to 31, ...) at most 2 rows name the same one
- route_weights: float32 [8192, 4], P('sp'), may hold values from 0.2 to 1
- w_gate: bfloat16 [64, 1024, 2048], P('sp', 'tp'), may hold values from -0.125 to 0.125
- w_up: bfloat16 [64, 1024, 2048], P('sp', 'tp'), may hold values from -0.125 to 0.125
- w_down: bfloat16 [64, 1024, 2048], P('sp', None, 'tp'), may hold values from -0.1875 to 0.1875
- shared_gate: bfloat16 [1024, 2048], P('tp'), may hold values from -0.125 to 0.125
- shared_up: bfloat16 [1024, 2048], P('tp'), may hold values from -0.125 to 0.125
- shared_down: bfloat16 [1024, 2048], P(None, 'tp'), may hold values from -0.1875 to 0.1875
Outputs:
- layer_out: bfloat16 [8192, 2048], P('sp', 'tp')
The draws below stay inside these ranges and needn't reach their ends.
Inputs may be any that keep to these rules, and one draw needn't show every extreme that they name: `routes`: in each aligned block of 16 rows no expert is named in more than 2 rows, and some blocks reach 2; a row names 4 different experts.
All inputs are finite; a program needn't handle non-finite values.
Results may differ from the reference program's by a relative error of at most 0.014.
Values may be sent and summed in bfloat16 or wider, within the bound.
A program may use at most 64 MiB of HBM per device.

```python
import math
import jax
import jax.numpy as jnp
import numpy as np
from jax import lax

D = 2048
HEADS = 16
KV_HEADS = 4
HD = 64
WINDOW = 128
EXPERTS = 64
TOPK = 4
FE = 1024
FS = 1024
TOKENS = 8192
ROWS_DEV = 16
CAP = 2
N_SP = 32
N_TP = 16


def draw_queries(key, part):
    base_key = jax.random.fold_in(key, 1)
    base_draw = jax.random.truncated_normal(base_key, -6.0, 6.0, (TOKENS, HEADS, HD), jnp.float32)
    return base_draw.reshape(TOKENS, HEADS * HD).astype(jnp.bfloat16)


def draw_keys(key, part):
    base_key = jax.random.fold_in(key, 2)
    base_draw = jax.random.truncated_normal(base_key, -6.0, 6.0, (TOKENS, KV_HEADS, HD), jnp.float32)
    return base_draw.reshape(TOKENS, KV_HEADS * HD).astype(jnp.bfloat16)


def block_levels(stream_key, extent, pieces, smallest, high):
    def one(dim, blocks):
        heights = jax.random.uniform(jax.random.fold_in(jax.random.fold_in(stream_key, 6), dim), (blocks,), jnp.float32, smallest / len(pieces), high / len(pieces))
        return jnp.repeat(jnp.exp(heights), extent[dim] // blocks).reshape((-1,) + (1,) * (len(extent) - dim - 1))

    factor_of = one(*pieces[0])
    for cut in pieces[1:]:
        factor_of = factor_of * one(*cut)
    return factor_of


def deal_out(stream_key, own, number, rows, amount, top, reach, lean):
    order = jax.random.permutation(stream_key, amount)
    packed, usual = portions_of(amount, rows * top, reach, lean, True), portions_of(amount, rows * top, reach, lean, False)
    places = jnp.arange(amount)

    def named(sizes, rotation):
        used = int((sizes > 0).sum())
        fixed = max(1, used // 4)
        passed = fixed + (places - fixed + rotation * (used - fixed)) % max(1, amount - fixed)
        return jnp.zeros((amount,), jnp.int32).at[order[jnp.where(places < fixed, places, passed)]].set(jnp.asarray(sizes, jnp.int32))

    sizes = jnp.where(number % 4 == 0, named(packed, number // 4), named(usual, number - number // 4 - 1))
    mixed = jax.random.permutation(jax.random.fold_in(own, 3), amount)
    giver, taker = mixed[0:amount // 2 * 2:2], mixed[1:amount // 2 * 2:2]
    room = jnp.minimum(sizes[giver] - 1, reach - sizes[taker]) // 2
    room = jnp.where((giver == order[0]) | (taker == order[0]) | (sizes[taker] == 0), 0, jnp.maximum(room, 0))
    passed = jax.random.randint(jax.random.fold_in(own, 4), (amount // 2,), 0, 1 << 20) % (room + 1)
    sizes = sizes.at[giver].add(-passed).at[taker].add(passed)
    items = jnp.searchsorted(jnp.cumsum(sizes), jnp.arange(rows * top), side="right").astype(jnp.int32)
    grid = items.reshape(top, rows).T
    grid = grid[jax.random.permutation(jax.random.fold_in(own, 1), rows)]
    rotation = jax.random.randint(jax.random.fold_in(own, 2), (rows, 1), 0, top)
    return jnp.take_along_axis(grid, (jnp.arange(top)[None, :] + rotation) % top, axis=1)


def portions_of(amount, total, bound, skew, full):
    portions = [(1 << 20) // math.isqrt(grade ** skew) + 1 for grade in range(1, amount + 1)]
    largest = bound if full else min(bound, max(-(-total // amount), total * portions[0] // sum(portions)))
    least = 1 if total - largest >= amount - 1 else 0
    given, surplus = [largest] + [least] * (amount - 1), total - largest - least * (amount - 1)
    while surplus > 0:
        candidates = [i for i in range(1, amount) if given[i] < largest] or [i for i in range(1, amount) if given[i] < bound]
        mass, left = sum([portions[i] for i in candidates]), surplus
        for i in candidates:
            addition = min(bound - given[i], max(1, left * portions[i] // mass), surplus)
            given[i] = given[i] + addition
            surplus = surplus - addition
    return np.array(given)


def bell_draw(rng, dims, scale, reach, cuts=(), dtype=jnp.bfloat16):
    level = block_levels(rng, dims, cuts, -0.22, 0.18) if cuts else 1.0
    result = jax.random.normal(rng, dims, jnp.float32) * scale * level
    return jnp.minimum(jnp.maximum(result, -reach), reach).astype(dtype)


def setup_inputs(seed: int = 0) -> dict:
    arg_keys = jax.random.split(jax.random.key(seed), 16)
    queries = draw_queries(jax.random.fold_in(arg_keys[15], 71), 0)
    keys = draw_keys(jax.random.fold_in(arg_keys[15], 71), 0)
    values = bell_draw(arg_keys[2], (TOKENS, KV_HEADS * HD), 1.0, 6.0, ((0, 32),))
    sink = jnp.clip(3.0 + 3.0 * jax.random.uniform(arg_keys[3], (HEADS,), jnp.float32) ** block_levels(arg_keys[3], (HEADS,), ((0, 16),), -0.2, 0.2), 3.0, 6.0)
    w_out = bell_draw(arg_keys[4], (HEADS * HD, D), (HEADS * HD) ** -0.5, 0.1875, ((0, 16),))
    stream = bell_draw(arg_keys[5], (TOKENS, D), 1.0, 6.0, ((0, 512),))
    gain = jnp.clip(1.0 + 0.18 * jax.random.normal(arg_keys[6], (D,), jnp.float32), 0.099609375, 1.8984375).astype(jnp.bfloat16)
    routes_keys = jax.random.split(jax.random.fold_in(arg_keys[7], 1), TOKENS // ROWS_DEV)
    routes_turns = jax.random.permutation(jax.random.fold_in(arg_keys[7], 3), TOKENS // ROWS_DEV)
    routes = jax.vmap(lambda own, number: deal_out(jax.random.fold_in(arg_keys[7], 2), own, number, ROWS_DEV, EXPERTS, TOPK, CAP, 2))(routes_keys, routes_turns).reshape((TOKENS, TOPK))
    route_weights = jnp.clip(0.2 + 0.8 * jax.random.uniform(arg_keys[8], (TOKENS, TOPK), jnp.float32) ** block_levels(arg_keys[8], (TOKENS, TOPK), ((0, 32),), -0.2, 0.2), 0.2, 1.0)
    w_gate = bell_draw(arg_keys[9], (EXPERTS, FE, D), D ** -0.5, 0.125, ((0, 32), (1, 16)))
    w_up = bell_draw(arg_keys[10], (EXPERTS, FE, D), D ** -0.5, 0.125, ((0, 32), (1, 16)))
    w_down = bell_draw(arg_keys[11], (EXPERTS, FE, D), FE ** -0.5, 0.1875, ((0, 32), (2, 16)))
    shared_gate = bell_draw(arg_keys[12], (FS, D), D ** -0.5, 0.125, ((0, 16),))
    shared_up = bell_draw(arg_keys[13], (FS, D), D ** -0.5, 0.125, ((0, 16),))
    shared_down = bell_draw(arg_keys[14], (FS, D), FS ** -0.5, 0.1875, ((1, 16),))
    return dict(queries=queries, keys=keys, values=values, sink=sink, w_out=w_out, stream=stream, gain=gain, routes=routes, route_weights=route_weights, w_gate=w_gate, w_up=w_up, w_down=w_down, shared_gate=shared_gate, shared_up=shared_up, shared_down=shared_down)


NORM_EPS = 1e-05

def attention_part(queries, keys, values, sink):
    group = HEADS // KV_HEADS
    blocks = TOKENS // WINDOW
    query_heads = queries.astype(jnp.float32).reshape(blocks, WINDOW, KV_HEADS, group, HD)

    def banded(source):
        padded = jnp.pad(source.astype(jnp.float32).reshape(TOKENS, KV_HEADS, HD), ((WINDOW, WINDOW), (0, 0), (0, 0)))
        framed = padded.reshape(blocks + 2, WINDOW, KV_HEADS, HD)
        return jnp.concatenate([framed[:-2], framed[1:-1], framed[2:]], axis=1)
    key_band = banded(keys)
    value_band = banded(values)
    scores = jnp.einsum('nqkgd,njkd->nkgqj', query_heads, key_band, precision=lax.Precision.HIGHEST) * HD ** (-0.5)
    query_pos = jnp.arange(blocks)[:, None, None] * WINDOW + jnp.arange(WINDOW)[None, :, None]
    key_pos = jnp.arange(blocks)[:, None, None] * WINDOW - WINDOW + jnp.arange(3 * WINDOW)[None, None, :]
    allowed = (jnp.abs(query_pos - key_pos) <= WINDOW) & (key_pos >= 0) & (key_pos < TOKENS)
    scores = jnp.where(allowed[:, None, None], scores, -jnp.inf)
    sink_level = sink.astype(jnp.float32).reshape(1, KV_HEADS, group, 1, 1)
    row_peak = jnp.maximum(scores.max(-1, keepdims=True), sink_level)
    probabilities = jnp.exp(scores - row_peak)
    denominator = probabilities.sum(-1, keepdims=True) + jnp.exp(sink_level - row_peak)
    rounded = lax.optimization_barrier((probabilities / denominator).astype(jnp.bfloat16)).astype(jnp.float32)
    attended = jnp.einsum('nkgqj,njkd->nqkgd', rounded, value_band, precision=lax.Precision.HIGHEST)
    return attended.astype(jnp.bfloat16).reshape(TOKENS, HEADS * HD)

def routed_part(normed, routes, route_weights, w_gate, w_up, w_down):
    most_rows = N_SP * N_TP * CAP
    flat_routes = routes.reshape(-1).astype(jnp.int32)
    flat_weights = route_weights.reshape(-1).astype(jnp.float32)
    sorted_ids = jnp.argsort(flat_routes, stable=True).astype(jnp.int32)
    counts = lax.optimization_barrier(jnp.sum((flat_routes[:, None] == jnp.arange(EXPERTS)[None, :]).astype(jnp.int32), axis=0))
    starts = (jnp.cumsum(counts) - counts).astype(jnp.int32)
    padded = jnp.concatenate([sorted_ids, jnp.zeros((most_rows,), jnp.int32)])

    def one_expert(accumulated, expert):
        picked = lax.dynamic_slice(padded, (starts[expert].astype(jnp.int32),), (most_rows,))
        is_valid = jnp.arange(most_rows) < counts[expert]
        token_ids = (picked // TOPK).astype(jnp.int32)
        picked_rows = normed[token_ids]
        gate_act = jnp.dot(picked_rows, w_gate[expert].T, preferred_element_type=jnp.float32)
        up_act = jnp.dot(picked_rows, w_up[expert].T, preferred_element_type=jnp.float32)
        hidden = (jax.nn.silu(gate_act) * up_act).astype(jnp.bfloat16)
        expert_out = jnp.dot(hidden, w_down[expert], preferred_element_type=jnp.float32)
        expert_out = lax.optimization_barrier(expert_out.astype(jnp.bfloat16)).astype(jnp.float32)
        scale_col = jnp.where(is_valid, flat_weights[picked], 0.0).astype(jnp.float32)
        return (accumulated.at[token_ids].add(expert_out * scale_col[:, None]), None)
    total_init = jnp.zeros((TOKENS, D), jnp.float32)
    routed, unused = lax.scan(one_expert, total_init, jnp.arange(EXPERTS))
    return routed

def reference(queries, keys, values, sink, w_out, stream, gain, routes, route_weights, w_gate, w_up, w_down, shared_gate, shared_up, shared_down):
    attended = attention_part(queries, keys, values, sink)
    projected = jnp.dot(attended, w_out, preferred_element_type=jnp.float32)
    mixed_rows = (stream.astype(jnp.float32) + projected).astype(jnp.bfloat16)
    wide_rows = mixed_rows.astype(jnp.float32)
    scale_rows = lax.rsqrt(lax.optimization_barrier(jnp.mean(wide_rows * wide_rows, axis=-1, keepdims=True)) + NORM_EPS)
    normed = (wide_rows * scale_rows * gain.astype(jnp.float32)).astype(jnp.bfloat16)
    routed = routed_part(normed, routes, route_weights, w_gate, w_up, w_down)
    shared_gate_act = jnp.dot(normed, shared_gate.T, preferred_element_type=jnp.float32)
    shared_up_act = jnp.dot(normed, shared_up.T, preferred_element_type=jnp.float32)
    shared_hidden = (jax.nn.silu(shared_gate_act) * shared_up_act).astype(jnp.bfloat16)
    shared_out = jnp.dot(shared_hidden, shared_down, preferred_element_type=jnp.float32)
    return (wide_rows + routed + shared_out).astype(jnp.bfloat16)
```

```python
import functools

import jax
import jax.numpy as jnp
from jax import lax
from jax.experimental import pallas as pl
from jax.experimental.pallas import tpu as pltpu
from jax.sharding import PartitionSpec as P

HD = 64
WINDOW = 128
CAP = 2
NX = 4
Z_ORDER = (0, 1, 4, 5, 3, 6, 2, 7)
NORM_EPS = 1e-05
BF = jnp.bfloat16
F32 = jnp.float32

NT = (((1,), (1,)), ((), ()))
TN = (((0,), (0,)), ((), ()))


def dot(a, b, dims=(((1,), (0,)), ((), ()))):
    return lax.dot_general(a, b, dims, preferred_element_type=F32)


def kernel(
    q_ref,
    k_ref,
    v_ref,
    sink_ref,
    w_out_ref,
    stream_ref,
    gain_ref,
    routes_ref,
    rw_ref,
    w_gate_ref,
    w_up_ref,
    w_down_ref,
    sg_ref,
    su_ref,
    sd_ref,
    out_ref,
    wcol,
    scol,
    halo,
    abuf,
    sbuf,
    gbuf,
    obuf,
    hs,
    hbuf,
    ybuf,
    rbuf,
    ptab,
    ctab,
    stab,
    wexp,
    wdt,
    resid,
    shared_out,
    w_sem,
    st_sem,
    halo_send,
    halo_recv,
    a_send,
    a_recv,
    d_send,
    d_recv,
    r_send,
    r_recv,
    ts_send,
    ts_recv,
    t_send,
    t_recv,
    hs_send,
    hs_recv,
    h_send,
    h_recv,
    *,
    kv_group,
    order,
    nx,
):
    tok, hd = q_ref.shape
    d_model = stream_ref.shape[1]
    rows_dev = stream_ref.shape[0]
    n_tp = lax.axis_size("tp")
    n_sp = lax.axis_size("sp")
    ny = n_tp // 2
    nz = n_sp // nx
    dc = d_model // n_tp
    exp_dev, fh = w_gate_ref.shape[0], w_gate_ref.shape[1]
    experts = exp_dev * n_sp
    topk = routes_ref.shape[0]
    slots = n_tp * CAP
    n_chunk = len(order) // 2 if len(order) > 2 else len(order)
    zc = len(order) // n_chunk
    crow = zc * nx * slots
    sp = lax.axis_index("sp")
    tp = lax.axis_index("tp")
    y, c = tp // 2, tp % 2
    z, x = sp // nx, sp % nx
    half = ny // 2

    def cols(t):
        return pl.ds(pl.multiple_of(t * dc, dc), dc)

    def units(t):
        return pl.ds(pl.multiple_of(t * fh, fh), fh)

    def chip(dy):
        return lax.rem(y + dy + ny, ny)

    def remote(src, dst, send, recv, **device):
        return pltpu.make_async_remote_copy(
            src_ref=src,
            dst_ref=dst,
            send_sem=send,
            recv_sem=recv,
            device_id=device,
            device_id_type=pl.DeviceIdType.MESH,
        )

    def wait_for(ref, sem):
        pltpu.make_async_copy(ref, ref, sem).wait()

    barrier = pltpu.get_barrier_semaphore()

    def greet_tp(i, carry):
        pl.semaphore_signal(barrier, inc=1, device_id={"tp": lax.rem(tp + i, n_tp)})
        return carry

    def greet_sp(i, carry):
        pl.semaphore_signal(barrier, inc=1, device_id={"sp": lax.rem(sp + i, n_sp)})
        return carry

    lax.fori_loop(1, n_tp, greet_tp, 0)
    lax.fori_loop(1, n_sp, greet_sp, 0)

    row_e = lax.broadcasted_iota(jnp.int32, (experts, tok), 0)
    hit_t = jnp.zeros((experts, tok), F32)
    weight_t = jnp.zeros((experts, tok), F32)
    for k in range(topk):
        hit = row_e == routes_ref[k : k + 1, :]
        hit_t = jnp.where(hit, 1.0, hit_t)
        weight_t = jnp.where(hit, rw_ref[k : k + 1, :], weight_t)
    early = lax.broadcasted_iota(jnp.int32, (tok, tok), 0)
    late = lax.broadcasted_iota(jnp.int32, (tok, tok), 1)
    before = (early < late) & (early // rows_dev == late // rows_dev)
    rank_t = dot(hit_t.astype(BF), jnp.where(before, 1.0, 0.0).astype(BF))
    slot_t = jnp.where(hit_t > 0, rank_t, -1.0)
    stab[...] = slot_t
    slot_row = lax.broadcasted_iota(jnp.int32, (slots, tok), 0)
    slot_tok = lax.broadcasted_iota(jnp.int32, (slots, tok), 1)
    in_block = (slot_row // CAP) == (slot_tok // rows_dev)
    slot_rank = jnp.where(in_block, slot_row % CAP, -2).astype(F32)

    def table_rows(e, carry):
        line = stab[pl.ds(e, 1), :]
        ptab[pl.ds(pl.multiple_of(e * slots, slots), slots), :] = jnp.where(
            line == slot_rank, 1.0, 0.0
        ).astype(BF)
        return carry

    lax.fori_loop(0, experts, table_rows, 0)

    pl.semaphore_wait(barrier, n_tp - 1 + n_sp - 1)

    head_kv = tp // kv_group
    pair = pl.ds(pl.multiple_of((head_kv // 2) * 2 * hd, 2 * hd), 2 * hd)
    last, first = sp == n_sp - 1, sp == 0
    to_next = lax.rem(sp + 1, n_sp)
    to_prev = lax.rem(sp + n_sp - 1, n_sp)

    def halo_copy(i):
        src = (k_ref, v_ref)[i % 2]
        rows = pl.ds(tok - WINDOW, WINDOW) if i < 2 else pl.ds(0, WINDOW)
        return remote(
            src.at[rows, pair],
            halo.at[i],
            halo_send.at[i],
            halo_recv.at[i],
            sp=to_next if i < 2 else to_prev,
        )

    @pl.when(jnp.logical_not(last))
    def _():
        halo_copy(0).start()
        halo_copy(1).start()

    @pl.when(jnp.logical_not(first))
    def _():
        halo_copy(2).start()
        halo_copy(3).start()

    def send_cols(i, carry):
        t = lax.rem(tp + i, n_tp)
        remote(w_out_ref.at[:, cols(t)], wcol.at[tp], w_sem.at[0], w_sem.at[1], tp=t).start()
        remote(stream_ref.at[:, cols(t)], scol.at[tp], st_sem.at[0], st_sem.at[1], tp=t).start()
        return carry

    lax.fori_loop(1, n_tp, send_cols, 0)
    wcol[tp] = w_out_ref[:, cols(tp)]
    scol[tp] = stream_ref[:, cols(tp)]

    @pl.when(first)
    def _():
        halo[0] = jnp.zeros(halo.shape[1:], BF)
        halo[1] = jnp.zeros(halo.shape[1:], BF)

    @pl.when(last)
    def _():
        halo[2] = jnp.zeros(halo.shape[1:], BF)
        halo[3] = jnp.zeros(halo.shape[1:], BF)

    @pl.when(jnp.logical_not(first))
    def _():
        halo_copy(0).wait_recv()
        halo_copy(1).wait_recv()

    @pl.when(jnp.logical_not(last))
    def _():
        halo_copy(2).wait_recv()
        halo_copy(3).wait_recv()

    odd = head_kv % 2
    lane = lax.broadcasted_iota(jnp.int32, (tok, 2 * hd), 1)
    query = q_ref[...]
    query = jnp.concatenate([query, query], axis=1)
    query = jnp.where(lane // hd == odd, query, jnp.zeros_like(query))
    sink = sink_ref[0:1, 0:1]
    key_i = lax.broadcasted_iota(jnp.int32, (WINDOW, WINDOW), 0)
    query_i = lax.broadcasted_iota(jnp.int32, (WINDOW, WINDOW), 1)
    blocks = tok // WINDOW
    for n in range(blocks):
        q_n = query[n * WINDOW : (n + 1) * WINDOW]
        parts = []
        for j in (-1, 0, 1):
            b = n + j
            if b < 0:
                key, value = halo[0], halo[1]
                allowed = (query_i <= key_i) & jnp.logical_not(first)
            elif b == blocks:
                key, value = halo[2], halo[3]
                allowed = (key_i <= query_i) & jnp.logical_not(last)
            else:
                rows = pl.ds(b * WINDOW, WINDOW)
                key, value = k_ref[rows, pair], v_ref[rows, pair]
                allowed = (query_i <= key_i, None, key_i <= query_i)[j + 1]
            score = dot(key, q_n, NT) * (hd**-0.5)
            if allowed is not None:
                score = jnp.where(allowed, score, -jnp.inf)
            parts.append((score, value))
        peak = jnp.maximum(sink, jnp.max(parts[0][0], axis=0, keepdims=True))
        for score, _v in parts[1:]:
            peak = jnp.maximum(peak, jnp.max(score, axis=0, keepdims=True))
        exps = [jnp.exp(score - peak) for score, _v in parts]
        total = jnp.exp(sink - peak)
        for e in exps:
            total = total + jnp.sum(e, axis=0, keepdims=True)
        mix = None
        for e, (_s, value) in zip(exps, parts):
            prob = (e / total).astype(BF)
            term = dot(value, prob, TN)
            mix = term if mix is None else mix + term
        mine = jnp.where(odd == 0, mix[:hd], mix[hd:])
        abuf[tp, :, n * WINDOW : (n + 1) * WINDOW] = mine.astype(BF)

    def peer_of(t):
        return 2 * (t // 2) + 1 - t % 2

    partner = peer_of(tp)

    def to_partner(t):
        return remote(abuf.at[t], abuf.at[t], a_send, a_recv.at[t], tp=partner)

    far = []
    for h in range(half, 0, -1):
        far.append(h)
        if h != half:
            far.append(-h)
    for h in far:
        remote(
            abuf.at[tp], abuf.at[tp], a_send, a_recv.at[tp], tp=2 * chip(h) + c
        ).start()
    to_partner(tp).start()

    gain = gain_ref[...].astype(F32)
    for e in range(exp_dev):
        wexp[e, :fh, :] = (w_gate_ref[e].astype(F32) * gain).astype(BF)
        wexp[e, fh:, :] = (w_up_ref[e].astype(F32) * gain).astype(BF)
    wexp[exp_dev, :fh, :] = (sg_ref[...].astype(F32) * gain).astype(BF)
    wexp[exp_dev, fh:, :] = (su_ref[...].astype(F32) * gain).astype(BF)

    for h in reversed(far):
        t = 2 * chip(h) + c
        wait_for(abuf.at[t], a_recv.at[t])
        to_partner(t).start()

    for e in range(exp_dev):
        wdt[e] = w_down_ref[e].astype(F32).T.astype(BF)
    wdt[exp_dev] = sd_ref[...].astype(F32).T.astype(BF)

    wait_for(wcol.at[pl.ds(0, n_tp - 1)], w_sem.at[1])
    wait_for(scol.at[pl.ds(0, n_tp - 1)], st_sem.at[1])
    for i in range(ny):
        t = 2 * chip(i) + 1 - c
        wait_for(abuf.at[t], a_recv.at[t])
    projected = dot(
        abuf[...].reshape(n_tp * hd, tok), wcol[...].reshape(n_tp * hd, dc), TN
    )
    mixed = (scol[...].reshape(tok, dc).astype(F32) + projected).astype(BF)
    resid[...] = mixed
    sbuf[:, cols(tp)] = mixed

    def dest(i, j):
        return lax.rem(z - order[i] + nz, nz) * nx + lax.rem(x + j, nx)

    def source(i, j):
        return lax.rem(z + order[i], nz) * nx + lax.rem(x + j, nx)

    def spot(pos):
        return pl.ds(pl.multiple_of(pos * slots, slots), slots)

    def chunk_rows(k):
        return pl.ds(pl.multiple_of(k * crow, crow), crow)

    pieces = min(4, n_sp)
    span = experts // pieces
    for part in range(pieces):
        rows = dot(ptab[part * span * slots : (part + 1) * span * slots, :], mixed)
        count = span // exp_dev
        obuf[part * count : (part + 1) * count] = rows.astype(BF).reshape(
            count, exp_dev, slots, dc
        )

    def ring_start(block, send, recv):
        for t in (2 * chip(1) + c, 2 * chip(-1) + c, partner):
            remote(block(tp), block(tp), send, recv(tp), tp=t).start()

    def ring_hop(block, send, recv, h):
        for sign in (1, -1):
            if h == half and sign == -1:
                continue
            t = 2 * chip(-sign * h) + c
            wait_for(block(t), recv(t))
            onto = 2 * chip(sign) + c
            if h < half - 1:
                remote(block(t), block(t), send, recv(t), tp=onto).start()
            elif h == half - 1:

                @pl.when(c == (0 if sign == 1 else 1))
                def _():
                    remote(block(t), block(t), send, recv(t), tp=onto).start()

            remote(block(t), block(t), send, recv(t), tp=partner).start()

    def ring_end(block, recv):
        for i in range(ny):
            t = 2 * chip(i) + 1 - c
            wait_for(block(t), recv(t))

    tok_shared = (
        lambda t: sbuf.at[:, cols(t)],
        ts_send,
        lambda t: ts_recv.at[t],
    )
    hid_shared = (
        lambda t: hs.at[units(t), :],
        hs_send,
        lambda t: hs_recv.at[t],
    )

    def tok_ring(k):
        return (
            lambda t: gbuf.at[:, chunk_rows(k), cols(t)],
            t_send.at[k],
            lambda t: t_recv.at[k, t],
        )

    def hid_ring(k):
        return (
            lambda t: hbuf.at[:, units(t), chunk_rows(k)],
            h_send.at[k],
            lambda t: h_recv.at[k, t],
        )

    def send_rows(i, j):
        d = dest(i, j)
        return remote(
            obuf.at[d],
            gbuf.at[:, spot(i * nx + x), cols(tp)],
            d_send,
            d_recv.at[i // zc],
            sp=d,
        )

    for i in range(len(order)):
        for j in range(nx):
            if i or j:
                send_rows(i, j).start()
    gbuf[:, spot(x), cols(tp)] = obuf[sp]
    ring_start(*tok_shared)

    def rows_arrived(k):
        count = zc * nx - (1 if k == 0 else 0)
        wait_for(
            gbuf.at[:, pl.ds(0, count * slots), cols(tp)],
            d_recv.at[k],
        )

    slot_c = slot_t.T.astype(BF)
    weight_c = weight_t.T.astype(BF)
    width = min(512, experts * slots)
    for part in range(experts * slots // width):
        m = lax.broadcasted_iota(jnp.int32, (experts, width), 1) + part * width
        e_i = lax.broadcasted_iota(jnp.int32, (experts, width), 0)
        spread = jnp.where(m // slots == e_i, 1.0, 0.0).astype(BF)
        m2 = lax.broadcasted_iota(jnp.int32, (tok, width), 1) + part * width
        r2 = lax.broadcasted_iota(jnp.int32, (tok, width), 0)
        want = jnp.where((m2 % slots) // CAP == r2 // rows_dev, m2 % CAP, -2).astype(F32)
        table = jnp.where(dot(slot_c, spread) == want, dot(weight_c, spread), 0.0)
        ctab[:, part * width : (part + 1) * width] = table.astype(BF)

    def hidden_of(rows, e):
        wide = rows.astype(F32)
        squares = wide * wide
        part = squares[:, :128]
        for i in range(1, d_model // 128):
            part = part + squares[:, i * 128 : (i + 1) * 128]
        total = jnp.sum(part.T, axis=0, keepdims=True)
        scale = lax.rsqrt(total / d_model + NORM_EPS)
        acts = dot(wexp[e], rows, NT) * scale
        gate, up = acts[:fh], acts[fh:]
        return (gate / (1.0 + jnp.exp(-gate)) * up).astype(BF)

    def up_shared():
        hs[units(tp), :] = hidden_of(sbuf[...], exp_dev)

    def up_chunk(k):
        for e in range(exp_dev):
            hbuf[e, units(tp), chunk_rows(k)] = hidden_of(gbuf[e, chunk_rows(k), :], e)

    def down_chunk(k):
        for e in range(exp_dev):
            res = dot(wdt[e], hbuf[e, :, chunk_rows(k)])
            ybuf[e, chunk_rows(k), :] = res.T.astype(BF)

    def give_back(i, j):
        s = source(i, j)
        pos = i * nx + lax.rem(x + j, nx)
        return remote(ybuf.at[:, spot(pos), :], rbuf.at[sp], r_send, r_recv, sp=s)

    def return_chunk(k):
        for i in range(k * zc, (k + 1) * zc):
            for j in range(nx):
                if i or j:
                    give_back(i, j).start()
        if k == 0:
            rbuf[sp] = ybuf[:, spot(x), :]

    ring_hop(*tok_shared, 1)
    rows_arrived(0)
    ring_start(*tok_ring(0))
    for h in range(2, half + 1):
        ring_hop(*tok_shared, h)
        ring_hop(*tok_ring(0), h - 1)
    rows_arrived(1)
    ring_start(*tok_ring(1))
    ring_end(tok_shared[0], tok_shared[2])
    up_shared()
    ring_start(*hid_shared)
    ring_hop(*tok_ring(0), half)
    ring_end(tok_ring(0)[0], tok_ring(0)[2])
    up_chunk(0)
    ring_start(*hid_ring(0))
    for k in range(1, n_chunk):
        for h in range(1, half + 1):
            ring_hop(*tok_ring(k), h)
            if k == 1:
                ring_hop(*hid_shared, h)
            ring_hop(*hid_ring(k - 1), h)
        if k + 1 < n_chunk:
            rows_arrived(k + 1)
            ring_start(*tok_ring(k + 1))
        ring_end(tok_ring(k)[0], tok_ring(k)[2])
        up_chunk(k)
        ring_start(*hid_ring(k))
        ring_end(hid_ring(k - 1)[0], hid_ring(k - 1)[2])
        down_chunk(k - 1)
        return_chunk(k - 1)
        if k == 1:
            ring_end(hid_shared[0], hid_shared[2])
            shared_out[...] = dot(wdt[exp_dev], hs[...]).T
    for h in range(1, half + 1):
        ring_hop(*hid_ring(n_chunk - 1), h)
    ring_end(hid_ring(n_chunk - 1)[0], hid_ring(n_chunk - 1)[2])
    down_chunk(n_chunk - 1)
    return_chunk(n_chunk - 1)

    wait_for(wcol.at[pl.ds(0, n_tp - 1)], w_sem.at[0])
    wait_for(scol.at[pl.ds(0, n_tp - 1)], st_sem.at[0])

    @pl.when(jnp.logical_not(last))
    def _():
        halo_copy(0).wait_send()
        halo_copy(1).wait_send()

    @pl.when(jnp.logical_not(first))
    def _():
        halo_copy(2).wait_send()
        halo_copy(3).wait_send()

    wait_for(abuf.at[pl.ds(0, n_tp - 1)], a_send)
    wait_for(obuf.at[pl.ds(0, n_sp - 1)], d_send)
    wait_for(sbuf.at[:, pl.ds(0, (n_tp - 1) * dc)], ts_send)
    wait_for(hs.at[pl.ds(0, (n_tp - 1) * fh), :], hs_send)
    for k in range(n_chunk):
        wait_for(gbuf.at[:, chunk_rows(k), pl.ds(0, (n_tp - 1) * dc)], t_send.at[k])
        wait_for(hbuf.at[:, pl.ds(0, (n_tp - 1) * fh), chunk_rows(k)], h_send.at[k])
    wait_for(rbuf.at[pl.ds(0, n_sp - 1)], r_send)

    wait_for(rbuf.at[pl.ds(0, n_sp - 1)], r_recv)
    routed = dot(ctab[...], rbuf[...].reshape(experts * slots, dc))
    out_ref[...] = (resid[...].astype(F32) + routed + shared_out[...]).astype(BF)


def local(
    queries,
    keys,
    values,
    sink,
    w_out,
    stream,
    gain,
    routes,
    route_weights,
    w_gate,
    w_up,
    w_down,
    shared_gate,
    shared_up,
    shared_down,
    *,
    kv_group,
    order,
    nx,
):
    n_tp = lax.axis_size("tp")
    n_sp = lax.axis_size("sp")
    tok = queries.shape[0]
    rows, d_model = stream.shape
    dc = d_model // n_tp
    exp_dev, fh, _ = w_gate.shape
    experts = exp_dev * n_sp
    slots = n_tp * CAP
    n_rows = n_sp * slots
    n_chunk = len(order) // 2 if len(order) > 2 else len(order)
    vm = pltpu.VMEM
    dma = pltpu.SemaphoreType.DMA
    return pl.pallas_call(
        functools.partial(kernel, kv_group=kv_group, order=order, nx=nx),
        out_shape=jax.ShapeDtypeStruct((tok, dc), BF),
        in_specs=[pl.BlockSpec(memory_space=vm)] * 15,
        out_specs=pl.BlockSpec(memory_space=vm),
        scratch_shapes=[
            vm((n_tp, w_out.shape[0], dc), BF),
            vm((n_tp, rows, dc), BF),
            vm((4, WINDOW, 2 * HD), BF),
            vm((n_tp, HD, tok), BF),
            vm((tok, d_model), BF),
            vm((exp_dev, n_rows, d_model), BF),
            vm((n_sp, exp_dev, slots, dc), BF),
            vm((n_tp * fh, tok), BF),
            vm((exp_dev, n_tp * fh, n_rows), BF),
            vm((exp_dev, n_rows, dc), BF),
            vm((n_sp, exp_dev, slots, dc), BF),
            vm((experts * slots, tok), BF),
            vm((tok, experts * slots), BF),
            vm((experts, tok), F32),
            vm((exp_dev + 1, 2 * fh, d_model), BF),
            vm((exp_dev + 1, dc, n_tp * fh), BF),
            vm((tok, dc), BF),
            vm((tok, dc), F32),
            dma((2,)),
            dma((2,)),
            dma((4,)),
            dma((4,)),
            dma(()),
            dma((n_tp,)),
            dma(()),
            dma((n_chunk,)),
            dma(()),
            dma(()),
            dma(()),
            dma((n_tp,)),
            dma((n_chunk,)),
            dma((n_chunk, n_tp)),
            dma(()),
            dma((n_tp,)),
            dma((n_chunk,)),
            dma((n_chunk, n_tp)),
        ],
        compiler_params=pltpu.CompilerParams(
            collective_id=0, has_side_effects=True, vmem_limit_bytes=60 * 1024 * 1024
        ),
    )(
        queries,
        keys,
        values,
        sink.reshape(1, 1),
        w_out,
        stream,
        gain.reshape(1, d_model),
        routes.T,
        route_weights.T,
        w_gate,
        w_up,
        w_down,
        shared_gate,
        shared_up,
        shared_down,
    )


def solution(mesh, kv_group=4, order=Z_ORDER, nx=NX):
    placed = (
        P("sp", "tp"),
        P("sp", None),
        P("sp", None),
        P("tp"),
        P("tp", None),
        P(("sp", "tp"), None),
        P(),
        P("sp", None),
        P("sp", None),
        P("sp", "tp", None),
        P("sp", "tp", None),
        P("sp", None, "tp"),
        P("tp", None),
        P("tp", None),
        P(None, "tp"),
    )
    return jax.shard_map(
        functools.partial(local, kv_group=kv_group, order=order, nx=nx),
        mesh=mesh,
        in_specs=placed,
        out_specs=P("sp", "tp"),
        check_vma=False,
    )
```

```python
import collections
import contextlib
import functools

import jax
import jax.numpy as jnp
from jax import lax
from jax.experimental import pallas as pl
from jax.experimental.pallas import tpu as pltpu
from jax.sharding import PartitionSpec as P

HD = 64
WINDOW = 128
CAP = 2
NX = 4
NEAR = (0, 0, 1, 1, 1, 1, 1, 3)
DIRECT = 1
Z_ORDER = (1, 7, 2, 6, 3, 5, 4, 0)
NORM_EPS = 1e-05
mark = contextlib.nullcontext
BF = jnp.bfloat16
F32 = jnp.float32

NT = (((1,), (1,)), ((), ()))
TN = (((0,), (0,)), ((), ()))


def dot(a, b, dims=(((1,), (0,)), ((), ()))):
    return lax.dot_general(a, b, dims, preferred_element_type=F32)


def kernel(
    q_in,
    k_in,
    v_in,
    sink_in,
    w_out_in,
    stream_in,
    gain_in,
    routes_in,
    rw_in,
    w_gate_in,
    w_up_in,
    w_down_in,
    sg_in,
    su_in,
    sd_in,
    out_ref,
    q_ref,
    k_ref,
    v_ref,
    sink_ref,
    w_out_ref,
    stream_ref,
    gain_ref,
    routes_ref,
    rw_ref,
    w_gate_ref,
    w_up_ref,
    w_down_ref,
    sg_ref,
    su_ref,
    sd_ref,
    in_sem,
    wcol,
    scol,
    halo,
    abuf,
    sbuf,
    gbuf,
    obuf,
    hs,
    hbuf,
    ybuf,
    rbuf,
    ptab,
    ctab,
    stab,
    wexp,
    wdt,
    resid,
    shared_out,
    w_sem,
    wx_send,
    wx_recv,
    st_sem,
    halo_send,
    halo_recv,
    a_send,
    a_recv,
    d_send,
    d_recv,
    r_send,
    r_recv,
    ts_send,
    ts_recv,
    t_send,
    t_recv,
    hs_send,
    hs_recv,
    h_send,
    h_recv,
    *,
    kv_group,
    order,
    near,
    nx,
):
    hd, tok = q_ref.shape
    d_model = stream_ref.shape[1]
    rows_dev = stream_ref.shape[0]
    n_tp = lax.axis_size("tp")
    n_sp = lax.axis_size("sp")
    ny = n_tp // 2
    nz = n_sp // nx
    dc = d_model // n_tp
    exp_dev, fh = w_gate_ref.shape[0], w_gate_ref.shape[1]
    experts = exp_dev * n_sp
    topk = routes_ref.shape[0]
    slots = n_tp * CAP
    n_chunk = len(order)
    own_chunk = order.index(0)
    direct = [ny // 2 if k >= n_chunk - DIRECT else 0 for k in range(n_chunk)]
    crow = nx * slots
    sp = lax.axis_index("sp")
    tp = lax.axis_index("tp")
    y, c = tp // 2, tp % 2
    z, x = sp // nx, sp % nx
    half = ny // 2

    def cols(t):
        return pl.ds(pl.multiple_of(t * dc, dc), dc)

    def units(t):
        return pl.ds(pl.multiple_of(t * fh, fh), fh)

    def chip(dy):
        return lax.rem(y + dy + ny, ny)

    def remote(src, dst, send, recv, **device):
        return pltpu.make_async_remote_copy(
            src_ref=src,
            dst_ref=dst,
            send_sem=send,
            recv_sem=recv,
            device_id=device,
            device_id_type=pl.DeviceIdType.MESH,
        )

    def wait_for(ref, sem):
        pltpu.make_async_copy(ref, ref, sem).wait()

    pairs = (
        (q_in, q_ref),
        (k_in, k_ref),
        (v_in, v_ref),
        (sink_in, sink_ref),
        (w_out_in, w_out_ref),
        (stream_in, stream_ref),
        (gain_in, gain_ref),
        (routes_in, routes_ref),
        (rw_in, rw_ref),
        (w_gate_in, w_gate_ref),
        (w_up_in, w_up_ref),
        (w_down_in, w_down_ref),
        (sg_in, sg_ref),
        (su_in, su_ref),
        (sd_in, sd_ref),
    )

    def load(i):
        return pltpu.make_async_copy(pairs[i][0], pairs[i][1], in_sem.at[i])

    barrier = pltpu.get_barrier_semaphore()

    def greet_tp(i, carry):
        pl.semaphore_signal(barrier, inc=1, device_id={"tp": lax.rem(tp + i, n_tp)})
        return carry

    def greet_sp(i, carry):
        pl.semaphore_signal(barrier, inc=1, device_id={"sp": lax.rem(sp + i, n_sp)})
        return carry

    lax.fori_loop(1, n_tp, greet_tp, 0)
    lax.fori_loop(1, n_sp, greet_sp, 0)
    for i in (1, 2, 4, 5, 0, 3, 7, 8, 6, 9, 10, 12, 13, 11, 14):
        load(i).start()

    with mark("barrier"):
        pl.semaphore_wait(barrier, n_tp - 1 + n_sp - 1)

    head_kv = tp // kv_group
    pair = pl.ds(pl.multiple_of((head_kv // 2) * 2 * hd, 2 * hd), 2 * hd)
    last, first = sp == n_sp - 1, sp == 0
    to_next = lax.rem(sp + 1, n_sp)
    to_prev = lax.rem(sp + n_sp - 1, n_sp)

    def halo_copy(i):
        src = (k_ref, v_ref)[i % 2]
        rows = pl.ds(tok - WINDOW, WINDOW) if i < 2 else pl.ds(0, WINDOW)
        return remote(
            src.at[rows, pair],
            halo.at[i],
            halo_send.at[i],
            halo_recv.at[i],
            sp=to_next if i < 2 else to_prev,
        )

    share = w_out_ref.shape[0] // nx
    own_part = pl.ds(pl.multiple_of(x * share, share), share)

    def send_cols(i, carry):
        t = lax.rem(tp + i, n_tp)
        remote(
            w_out_ref.at[own_part, cols(t)], wcol.at[tp, own_part], w_sem.at[0], w_sem.at[1], tp=t
        ).start()
        return carry

    def send_stream(i, carry):
        t = lax.rem(tp + i, n_tp)
        remote(stream_ref.at[:, cols(t)], scol.at[tp], st_sem.at[0], st_sem.at[1], tp=t).start()
        return carry

    load(1).wait()
    load(2).wait()
    @pl.when(jnp.logical_not(last))
    def _():
        halo_copy(0).start()
        halo_copy(1).start()

    @pl.when(jnp.logical_not(first))
    def _():
        halo_copy(2).start()
        halo_copy(3).start()
    load(4).wait()
    lax.fori_loop(1, n_tp, send_cols, 0)
    load(5).wait()
    lax.fori_loop(1, n_tp, send_stream, 0)
    wcol[tp, own_part] = w_out_ref[own_part, cols(tp)]
    scol[tp] = stream_ref[:, cols(tp)]
    load(0).wait()
    load(3).wait()
    load(7).wait()
    load(8).wait()

    row_e = lax.broadcasted_iota(jnp.int32, (experts, tok), 0)
    hit_t = jnp.zeros((experts, tok), F32)
    weight_t = jnp.zeros((experts, tok), F32)
    for k in range(topk):
        hit = row_e == routes_ref[k : k + 1, :]
        hit_t = jnp.where(hit, 1.0, hit_t)
        weight_t = jnp.where(hit, rw_ref[k : k + 1, :], weight_t)
    early = lax.broadcasted_iota(jnp.int32, (tok, tok), 0)
    late = lax.broadcasted_iota(jnp.int32, (tok, tok), 1)
    before = (early < late) & (early // rows_dev == late // rows_dev)
    rank_t = dot(hit_t.astype(BF), jnp.where(before, 1.0, 0.0).astype(BF))
    slot_t = jnp.where(hit_t > 0, rank_t, -1.0)
    stab[...] = slot_t
    slot_row = lax.broadcasted_iota(jnp.int32, (slots, tok), 0)
    slot_tok = lax.broadcasted_iota(jnp.int32, (slots, tok), 1)
    in_block = (slot_row // CAP) == (slot_tok // rows_dev)
    slot_rank = jnp.where(in_block, slot_row % CAP, -2).astype(F32)

    def table_rows(e, carry):
        line = stab[pl.ds(e, 1), :]
        ptab[pl.ds(pl.multiple_of(e * slots, slots), slots), :] = jnp.where(
            line == slot_rank, 1.0, 0.0
        ).astype(BF)
        return carry

    lax.fori_loop(0, experts, table_rows, 0)

    @pl.when(first)
    def _():
        halo[0] = jnp.zeros(halo.shape[1:], BF)
        halo[1] = jnp.zeros(halo.shape[1:], BF)

    @pl.when(last)
    def _():
        halo[2] = jnp.zeros(halo.shape[1:], BF)
        halo[3] = jnp.zeros(halo.shape[1:], BF)

    with mark("halo_wait"):
        @pl.when(jnp.logical_not(first))
        def _():
            halo_copy(0).wait_recv()
            halo_copy(1).wait_recv()

        @pl.when(jnp.logical_not(last))
        def _():
            halo_copy(2).wait_recv()
            halo_copy(3).wait_recv()

    odd = head_kv % 2
    query = q_ref[...]
    empty = jnp.zeros_like(query)
    query = jnp.concatenate(
        [jnp.where(odd == 0, query, empty), jnp.where(odd == 0, empty, query)], axis=0
    )
    sink = sink_ref[0:1, 0:1]
    key_i = lax.broadcasted_iota(jnp.int32, (WINDOW, WINDOW), 0)
    query_i = lax.broadcasted_iota(jnp.int32, (WINDOW, WINDOW), 1)
    blocks = tok // WINDOW
    for n in range(blocks):
        q_n = query[:, n * WINDOW : (n + 1) * WINDOW]
        parts = []
        for j in (-1, 0, 1):
            b = n + j
            if b < 0:
                key, value = halo[0], halo[1]
                allowed = (query_i <= key_i) & jnp.logical_not(first)
            elif b == blocks:
                key, value = halo[2], halo[3]
                allowed = (key_i <= query_i) & jnp.logical_not(last)
            else:
                rows = pl.ds(b * WINDOW, WINDOW)
                key, value = k_ref[rows, pair], v_ref[rows, pair]
                allowed = (query_i <= key_i, None, key_i <= query_i)[j + 1]
            score = dot(key, q_n) * (hd**-0.5)
            if allowed is not None:
                score = jnp.where(allowed, score, -jnp.inf)
            parts.append((score, value))
        peak = jnp.maximum(sink, jnp.max(parts[0][0], axis=0, keepdims=True))
        for score, _v in parts[1:]:
            peak = jnp.maximum(peak, jnp.max(score, axis=0, keepdims=True))
        exps = [jnp.exp(score - peak) for score, _v in parts]
        total = jnp.exp(sink - peak)
        for e in exps:
            total = total + jnp.sum(e, axis=0, keepdims=True)
        mix = None
        for e, (_s, value) in zip(exps, parts):
            prob = (e / total).astype(BF)
            term = dot(value, prob, TN)
            mix = term if mix is None else mix + term
        mine = jnp.where(odd == 0, mix[:hd], mix[hd:])
        abuf[tp, :, n * WINDOW : (n + 1) * WINDOW] = mine.astype(BF)

    def peer_of(t):
        return 2 * (t // 2) + 1 - t % 2

    partner = peer_of(tp)

    def to_partner(t):
        return remote(abuf.at[t], abuf.at[t], a_send, a_recv.at[t], tp=partner)

    def to_chip(t, h):
        return remote(abuf.at[t], abuf.at[t], a_send, a_recv.at[t], tp=2 * chip(h) + c)

    for h in range(half, 0, -1):
        to_chip(tp, h).start()
        if h < half:
            to_chip(tp, -h).start()
    to_partner(tp).start()

    def w_along_x(j):
        part = wcol.at[:, own_part]
        to = z * nx + lax.rem(x + j, nx)
        return remote(part, part, wx_send.at[j - 1], wx_recv.at[j - 1], sp=to)

    with mark("w_wait"):
        wait_for(wcol.at[pl.ds(0, n_tp - 1), own_part], w_sem.at[1])
    for j in range(1, nx):
        w_along_x(j).start()

    for i in (6, 9, 10, 12, 13, 11, 14):
        load(i).wait()
    for i in range(d_model // 128):
        some = slice(i * 128, (i + 1) * 128)
        gain = gain_ref[i : i + 1, :].astype(F32)
        for e in range(exp_dev):
            wexp[e, :fh, some] = (w_gate_ref[e, :, some].astype(F32) * gain).astype(BF)
            wexp[e, fh:, some] = (w_up_ref[e, :, some].astype(F32) * gain).astype(BF)
        wexp[exp_dev, :fh, some] = (sg_ref[:, some].astype(F32) * gain).astype(BF)
        wexp[exp_dev, fh:, some] = (su_ref[:, some].astype(F32) * gain).astype(BF)

    with mark("att_wait"):
        for h in range(1, half + 1):
            for sign in (1, -1):
                if h == half and sign == -1:
                    continue
                t = 2 * chip(-sign * h) + c
                wait_for(abuf.at[t], a_recv.at[t])
                to_partner(t).start()

    for e in range(exp_dev):
        wdt[e] = w_down_ref[e].astype(F32).T.astype(BF)
    wdt[exp_dev] = sd_ref[...].astype(F32).T.astype(BF)

    with mark("att_wait2"):
        for j in range(1, nx):
            w_along_x(j).wait_recv()
        wait_for(scol.at[pl.ds(0, n_tp - 1)], st_sem.at[1])
        for i in range(ny):
            t = 2 * chip(i) + 1 - c
            wait_for(abuf.at[t], a_recv.at[t])
    projected = dot(
        abuf[...].reshape(n_tp * hd, tok), wcol[...].reshape(n_tp * hd, dc), TN
    )
    mixed = (scol[...].reshape(tok, dc).astype(F32) + projected).astype(BF)
    resid[...] = mixed
    sbuf[:, cols(tp)] = mixed

    def dest(i, j):
        return lax.rem(z - order[i] + nz, nz) * nx + lax.rem(x + j, nx)

    def source(i, j):
        return lax.rem(z + order[i], nz) * nx + lax.rem(x + j, nx)

    def spot(pos):
        return pl.ds(pl.multiple_of(pos * slots, slots), slots)

    def chunk_rows(k):
        return pl.ds(pl.multiple_of(k * crow, crow), crow)

    def ring_start(block, send, recv, near=0):
        for t in (2 * chip(1) + c, 2 * chip(-1) + c, partner)[2 if near else 0 :]:
            remote(block(tp), block(tp), send, recv(tp), tp=t).start()

    def pass_on(block, send, recv, h, sign, near=0):
        t = 2 * chip(-sign * h) + c
        onto = 2 * chip(sign) + c
        if near <= h < half - 1:
            remote(block(t), block(t), send, recv(t), tp=onto).start()
        elif near <= h == half - 1:

            @pl.when(c == (0 if sign == 1 else 1))
            def _():
                remote(block(t), block(t), send, recv(t), tp=onto).start()

        remote(block(t), block(t), send, recv(t), tp=partner).start()

    def ring_hop(block, send, recv, h, near=0):
        for sign in (1, -1):
            if h < half or sign == 1:
                t = 2 * chip(-sign * h) + c
                wait_for(block(t), recv(t))
                pass_on(block, send, recv, h, sign, near)

    def to_all(block, send, recv):
        for h in range(half, 0, -1):
            for sign in (1, -1):
                if h < half or sign == 1:
                    onto = 2 * chip(sign * h) + c
                    remote(block(tp), block(tp), send, recv(tp), tp=onto).start()
        remote(block(tp), block(tp), send, recv(tp), tp=partner).start()

    def ring_end(block, recv):
        for i in range(ny):
            t = 2 * chip(i) + 1 - c
            wait_for(block(t), recv(t))

    tok_shared = (
        lambda t: sbuf.at[:, cols(t)],
        ts_send,
        lambda t: ts_recv.at[t],
    )
    hid_shared = (
        lambda t: hs.at[units(t), :],
        hs_send,
        lambda t: hs_recv.at[t],
    )

    def tok_ring(k):
        return (
            lambda t: gbuf.at[:, chunk_rows(k), cols(t)],
            t_send.at[k],
            lambda t: t_recv.at[k, t],
        )

    def hid_ring(k):
        return (
            lambda t: hbuf.at[:, units(t), chunk_rows(k)],
            h_send.at[k],
            lambda t: h_recv.at[k, t],
        )

    ring_start(*tok_shared)
    pieces = min(4, n_sp)
    count = n_sp // pieces
    with mark("dispdot"):
        for part in range(pieces):
            size = count * exp_dev * slots
            rows = dot(ptab[part * size : (part + 1) * size, :], mixed)
            obuf[part * count : (part + 1) * count] = rows.astype(BF).reshape(
                count, exp_dev, slots, dc
            )

    def shown(n):
        return 2 * chip((n + 1) // 2 * (-1 if n % 2 else 1)) + c

    def send_rows(n, i):
        for j in range(nx):
            if i == own_chunk and j == 0:
                gbuf[:, spot(i * nx + x), cols(shown(n))] = obuf[n * n_sp + sp]
            else:
                d = dest(i, j)
                remote(
                    obuf.at[n * n_sp + d],
                    gbuf.at[:, spot(i * nx + x), cols(shown(n))],
                    d_send,
                    d_recv.at[i, n],
                    sp=d,
                ).start()

    def beside(h):
        return jnp.concatenate(
            [sbuf[:, cols(shown(2 * h - 1))], sbuf[:, cols(shown(2 * h))]], axis=1
        )

    def make_rows(h, at, blocks, both):
        size = exp_dev * slots
        some = pl.ds(pl.multiple_of(at * size, size), blocks * size)
        rows = dot(ptab[some, :], both)
        for n in (2 * h - 1, 2 * h):
            half_rows = rows[:, :dc] if n % 2 else rows[:, dc:]
            obuf[pl.ds(n * n_sp + at, blocks)] = half_rows.astype(BF).reshape(
                blocks, exp_dev, slots, dc
            )

    def rows_arrived(n, k):
        rows = (nx - (1 if k == own_chunk else 0)) * slots
        if rows:
            wait_for(gbuf.at[:, pl.ds(0, rows), cols(tp)], d_recv.at[k, n])

    def inject(h):
        both = beside(h)
        takers = [i for i in range(n_chunk) if near[i] >= h]
        if 2 * len(takers) > n_chunk:
            for part in range(pieces):
                make_rows(h, part * count, count, both)
        else:
            for i in takers:
                make_rows(h, lax.rem(z - order[i] + nz, nz) * nx, nx, both)
        for i in range(n_chunk):
            if h == 1 and i >= ahead:
                send_rows(0, i)
            if near[i] >= h:
                send_rows(2 * h - 1, i)
                send_rows(2 * h, i)

    ahead = min(4, n_chunk)
    for i in range(ahead):
        send_rows(0, i)

    slot_c = slot_t.T.astype(BF)
    weight_c = weight_t.T.astype(BF)
    width = min(512, experts * slots)
    for part in range(experts * slots // width):
        m = lax.broadcasted_iota(jnp.int32, (experts, width), 1) + part * width
        e_i = lax.broadcasted_iota(jnp.int32, (experts, width), 0)
        spread = jnp.where(m // slots == e_i, 1.0, 0.0).astype(BF)
        m2 = lax.broadcasted_iota(jnp.int32, (tok, width), 1) + part * width
        r2 = lax.broadcasted_iota(jnp.int32, (tok, width), 0)
        want = jnp.where((m2 % slots) // CAP == r2 // rows_dev, m2 % CAP, -2).astype(F32)
        table = jnp.where(dot(slot_c, spread) == want, dot(weight_c, spread), 0.0)
        ctab[:, part * width : (part + 1) * width] = table.astype(BF)

    def hidden_of(rows, e):
        wide = rows.astype(F32)
        squares = wide * wide
        part = squares[:, :128]
        for i in range(1, d_model // 128):
            part = part + squares[:, i * 128 : (i + 1) * 128]
        total = jnp.sum(part.T, axis=0, keepdims=True)
        scale = lax.rsqrt(total / d_model + NORM_EPS)
        acts = dot(wexp[e], rows, NT) * scale
        gate, up = acts[:fh], acts[fh:]
        return (gate / (1.0 + jnp.exp(-gate)) * up).astype(BF)

    def up_shared():
        ring_end(tok_shared[0], tok_shared[2])
        hs[units(tp), :] = hidden_of(sbuf[...], exp_dev)
        ring_start(*hid_shared)

    def up_chunk(k):
        ring_end(tok_ring(k)[0], tok_ring(k)[2])
        for e in range(exp_dev):
            hbuf[e, units(tp), chunk_rows(k)] = hidden_of(gbuf[e, chunk_rows(k), :], e)
        if direct[k]:
            to_all(*hid_ring(k))
        else:
            ring_start(*hid_ring(k))

    def down_shared():
        ring_end(hid_shared[0], hid_shared[2])
        shared_out[...] = dot(wdt[exp_dev], hs[...]).T

    def down_chunk(k):
        ring_end(hid_ring(k)[0], hid_ring(k)[2])
        for e in range(exp_dev):
            res = dot(wdt[e], hbuf[e, :, chunk_rows(k)])
            ybuf[e, chunk_rows(k), :] = res.T.astype(BF)
        return_chunk(k)

    def give_back(i, j):
        s = source(i, j)
        pos = i * nx + lax.rem(x + j, nx)
        return remote(ybuf.at[:, spot(pos), :], rbuf.at[sp], r_send, r_recv, sp=s)

    def return_chunk(k):
        for j in range(nx):
            if k == own_chunk and j == 0:
                rbuf[sp] = ybuf[:, spot(k * nx + x), :]
            else:
                give_back(k, j).start()

    def tok_in(k):
        rows_arrived(0, k)
        ring_start(*tok_ring(k), near[k])
        for h in range(1, near[k] + 1):
            for n, sign in ((2 * h - 1, 1), (2 * h, -1)):
                rows_arrived(n, k)
                pass_on(*tok_ring(k), h, sign, near[k])

    slots_of = collections.defaultdict(list)
    for h in range(1, half + 1):
        slots_of[h - 2].append((2, f"tokS_{h}", lambda h=h: ring_hop(*tok_shared, h)))
        slots_of[half - 2 + h].append((1, f"hidS_{h}", lambda h=h: ring_hop(*hid_shared, h)))
    slots_of[half - 2].append((3, "upS", up_shared))
    slots_of[2 * half - 2].append((4, "downS", down_shared))
    for h in range(1, max(half, 2)):
        slots_of[h - 2].append((3, f"inject{h}", lambda h=h: inject(h)))
    for k in range(n_chunk):
        up_at = k + half - 1
        slots_of[up_at - half + near[k]].append((2, f"in{k}", lambda k=k: tok_in(k)))
        for h in range(near[k] + 1, half + 1):
            slots_of[up_at - half + h].append(
                (2, f"tok{k}_{h}", lambda k=k, h=h: ring_hop(*tok_ring(k), h))
            )
        slots_of[up_at].append((3, f"up{k}", lambda k=k: up_chunk(k)))
        for h in range(1, half + 1):
            slots_of[up_at + (half if direct[k] else h)].append(
                (1, f"hid{k}_{h}", lambda k=k, h=h: ring_hop(*hid_ring(k), h, direct[k]))
            )
        slots_of[up_at + half].append((4, f"down{k}", lambda k=k: down_chunk(k)))
    for slot in sorted(slots_of):
        for _r, name, step in sorted(slots_of[slot], key=lambda item: item[0]):
            with mark(name):
                step()

    wait_for(wcol.at[pl.ds(0, n_tp - 1), own_part], w_sem.at[0])
    for j in range(1, nx):
        w_along_x(j).wait_send()
    wait_for(scol.at[pl.ds(0, n_tp - 1)], st_sem.at[0])

    @pl.when(jnp.logical_not(last))
    def _():
        halo_copy(0).wait_send()
        halo_copy(1).wait_send()

    @pl.when(jnp.logical_not(first))
    def _():
        halo_copy(2).wait_send()
        halo_copy(3).wait_send()

    wait_for(abuf.at[pl.ds(0, n_tp - 1)], a_send)
    count = sum((1 + 2 * near[i]) * (nx - (i == own_chunk)) for i in range(n_chunk))
    wait_for(obuf.at[pl.ds(0, count)], d_send)
    wait_for(sbuf.at[:, pl.ds(0, (n_tp - 1) * dc)], ts_send)
    wait_for(hs.at[pl.ds(0, (n_tp - 1) * fh), :], hs_send)
    for k in range(n_chunk):
        wait_for(
            gbuf.at[:, chunk_rows(k), pl.ds(0, (n_tp - 1 - 2 * near[k]) * dc)], t_send.at[k]
        )
        wait_for(hbuf.at[:, pl.ds(0, (n_tp - 1) * fh), chunk_rows(k)], h_send.at[k])
    wait_for(rbuf.at[pl.ds(0, n_sp - 1)], r_send)

    with mark("ret_wait"):
        wait_for(rbuf.at[pl.ds(0, n_sp - 1)], r_recv)
    with mark("combine"):
        routed = dot(ctab[...], rbuf[...].reshape(experts * slots, dc))
        out_ref[...] = (resid[...].astype(F32) + routed + shared_out[...]).astype(BF)


def local(
    queries,
    keys,
    values,
    sink,
    w_out,
    stream,
    gain,
    routes,
    route_weights,
    w_gate,
    w_up,
    w_down,
    shared_gate,
    shared_up,
    shared_down,
    *,
    kv_group,
    order,
    near,
    nx,
):
    n_tp = lax.axis_size("tp")
    n_sp = lax.axis_size("sp")
    tok = queries.shape[0]
    rows, d_model = stream.shape
    dc = d_model // n_tp
    exp_dev, fh, _ = w_gate.shape
    experts = exp_dev * n_sp
    slots = n_tp * CAP
    n_rows = n_sp * slots
    n_chunk = len(order)
    vm = pltpu.VMEM
    dma = pltpu.SemaphoreType.DMA
    inputs = (
        queries.T,
        keys,
        values,
        sink.reshape(1, 1),
        w_out,
        stream,
        gain.reshape(d_model // 128, 128),
        routes.T,
        route_weights.T,
        w_gate,
        w_up,
        w_down,
        shared_gate,
        shared_up,
        shared_down,
    )
    return pl.pallas_call(
        functools.partial(kernel, kv_group=kv_group, order=order, near=near, nx=nx),
        out_shape=jax.ShapeDtypeStruct((tok, dc), BF),
        in_specs=[pl.BlockSpec(memory_space=pl.ANY)] * 15,
        out_specs=pl.BlockSpec(memory_space=vm),
        scratch_shapes=[
            *[vm(a.shape, a.dtype) for a in inputs],
            dma((len(inputs),)),
            vm((n_tp, w_out.shape[0], dc), BF),
            vm((n_tp, rows, dc), BF),
            vm((4, WINDOW, 2 * HD), BF),
            vm((n_tp, HD, tok), BF),
            vm((tok, d_model), BF),
            vm((exp_dev, n_rows, d_model), BF),
            vm(((1 + 2 * max(near)) * n_sp, exp_dev, slots, dc), BF),
            vm((n_tp * fh, tok), BF),
            vm((exp_dev, n_tp * fh, n_rows), BF),
            vm((exp_dev, n_rows, dc), BF),
            vm((n_sp, exp_dev, slots, dc), BF),
            vm((experts * slots, tok), BF),
            vm((tok, experts * slots), BF),
            vm((experts, tok), F32),
            vm((exp_dev + 1, 2 * fh, d_model), BF),
            vm((exp_dev + 1, dc, n_tp * fh), BF),
            vm((tok, dc), BF),
            vm((tok, dc), F32),
            dma((2,)),
            dma((max(nx - 1, 1),)),
            dma((max(nx - 1, 1),)),
            dma((2,)),
            dma((4,)),
            dma((4,)),
            dma(()),
            dma((n_tp,)),
            dma(()),
            dma((n_chunk, 1 + 2 * max(near))),
            dma(()),
            dma(()),
            dma(()),
            dma((n_tp,)),
            dma((n_chunk,)),
            dma((n_chunk, n_tp)),
            dma(()),
            dma((n_tp,)),
            dma((n_chunk,)),
            dma((n_chunk, n_tp)),
        ],
        compiler_params=pltpu.CompilerParams(
            collective_id=0, has_side_effects=True, vmem_limit_bytes=60 * 1024 * 1024
        ),
    )(*inputs)


def solution(mesh, kv_group=4, order=Z_ORDER, near=NEAR, nx=NX):
    placed = (
        P("sp", "tp"),
        P("sp", None),
        P("sp", None),
        P("tp"),
        P("tp", None),
        P(("sp", "tp"), None),
        P(),
        P("sp", None),
        P("sp", None),
        P("sp", "tp", None),
        P("sp", "tp", None),
        P("sp", None, "tp"),
        P("tp", None),
        P("tp", None),
        P(None, "tp"),
    )
    return jax.shard_map(
        functools.partial(local, kv_group=kv_group, order=order, near=near, nx=nx),
        mesh=mesh,
        in_specs=placed,
        out_specs=P("sp", "tp"),
        check_vma=False,
    )
```

```python
import collections
import contextlib
import functools

import jax
import jax.numpy as jnp
from jax import lax
from jax.experimental import pallas as pl
from jax.experimental.pallas import tpu as pltpu
from jax.sharding import PartitionSpec as P

HD = 64
WINDOW = 128
CAP = 2
NX = 4
NEAR = (0, 0, 0, 1, 1, 1, 3, 3)
DIRECT = 0
Z_ORDER = (1, 2, 3, 6, 5, 4, 7, 0)
NORM_EPS = 1e-05
mark = contextlib.nullcontext
BF = jnp.bfloat16
F32 = jnp.float32

NT = (((1,), (1,)), ((), ()))
TN = (((0,), (0,)), ((), ()))


def dot(a, b, dims=(((1,), (0,)), ((), ()))):
    return lax.dot_general(a, b, dims, preferred_element_type=F32)


def kernel(
    q_in,
    k_in,
    v_in,
    sink_in,
    w_out_in,
    stream_in,
    gain_in,
    routes_in,
    rw_in,
    w_gate_in,
    w_up_in,
    w_down_in,
    sg_in,
    su_in,
    sd_in,
    out_ref,
    q_ref,
    k_ref,
    v_ref,
    sink_ref,
    w_out_ref,
    stream_ref,
    gain_ref,
    routes_ref,
    rw_ref,
    w_gate_ref,
    w_up_ref,
    w_down_ref,
    sg_ref,
    su_ref,
    sd_ref,
    in_sem,
    wcol,
    scol,
    halo,
    abuf,
    sbuf,
    gbuf,
    obuf,
    hs,
    hbuf,
    ybuf,
    rbuf,
    ptab,
    ctab,
    stab,
    wexp,
    wdt,
    resid,
    shared_out,
    w_sem,
    wx_send,
    wx_recv,
    st_sem,
    halo_send,
    halo_recv,
    a_send,
    a_recv,
    d_send,
    d_recv,
    r_send,
    r_recv,
    ts_send,
    ts_recv,
    t_send,
    t_recv,
    hs_send,
    hs_recv,
    h_send,
    h_recv,
    *,
    kv_group,
    order,
    near,
    nx,
):
    hd, tok = q_ref.shape
    d_model = stream_ref.shape[1]
    rows_dev = stream_ref.shape[0]
    n_tp = lax.axis_size("tp")
    n_sp = lax.axis_size("sp")
    ny = n_tp // 2
    nz = n_sp // nx
    dc = d_model // n_tp
    exp_dev, fh = w_gate_ref.shape[0], w_gate_ref.shape[1]
    experts = exp_dev * n_sp
    topk = routes_ref.shape[0]
    slots = n_tp * CAP
    n_chunk = len(order)
    own_chunk = order.index(0)
    direct = [ny // 2 if k >= n_chunk - DIRECT else 0 for k in range(n_chunk)]
    crow = nx * slots
    sp = lax.axis_index("sp")
    tp = lax.axis_index("tp")
    y, c = tp // 2, tp % 2
    z, x = sp // nx, sp % nx
    half = ny // 2

    def cols(t):
        return pl.ds(pl.multiple_of(t * dc, dc), dc)

    def units(t):
        return pl.ds(pl.multiple_of(t * fh, fh), fh)

    def chip(dy):
        return lax.rem(y + dy + ny, ny)

    def remote(src, dst, send, recv, **device):
        return pltpu.make_async_remote_copy(
            src_ref=src,
            dst_ref=dst,
            send_sem=send,
            recv_sem=recv,
            device_id=device,
            device_id_type=pl.DeviceIdType.MESH,
        )

    def wait_for(ref, sem):
        pltpu.make_async_copy(ref, ref, sem).wait()

    pairs = (
        (q_in, q_ref),
        (k_in, k_ref),
        (v_in, v_ref),
        (sink_in, sink_ref),
        (w_out_in, w_out_ref),
        (stream_in, stream_ref),
        (gain_in, gain_ref),
        (routes_in, routes_ref),
        (rw_in, rw_ref),
        (w_gate_in, w_gate_ref),
        (w_up_in, w_up_ref),
        (w_down_in, w_down_ref),
        (sg_in, sg_ref),
        (su_in, su_ref),
        (sd_in, sd_ref),
    )

    def load(i):
        return pltpu.make_async_copy(pairs[i][0], pairs[i][1], in_sem.at[i])

    barrier = pltpu.get_barrier_semaphore()

    def greet_tp(i, carry):
        pl.semaphore_signal(barrier, inc=1, device_id={"tp": lax.rem(tp + i, n_tp)})
        return carry

    def greet_sp(i, carry):
        pl.semaphore_signal(barrier, inc=1, device_id={"sp": lax.rem(sp + i, n_sp)})
        return carry

    lax.fori_loop(1, n_tp, greet_tp, 0)
    lax.fori_loop(1, n_sp, greet_sp, 0)
    for i in (1, 2, 4, 5, 0, 3, 7, 8, 6, 9, 10, 12, 13, 11, 14):
        load(i).start()

    with mark("barrier"):
        pl.semaphore_wait(barrier, n_tp - 1 + n_sp - 1)

    head_kv = tp // kv_group
    pair = pl.ds(pl.multiple_of((head_kv // 2) * 2 * hd, 2 * hd), 2 * hd)
    last, first = sp == n_sp - 1, sp == 0
    to_next = lax.rem(sp + 1, n_sp)
    to_prev = lax.rem(sp + n_sp - 1, n_sp)

    def halo_copy(i):
        src = (k_ref, v_ref)[i % 2]
        rows = pl.ds(tok - WINDOW, WINDOW) if i < 2 else pl.ds(0, WINDOW)
        return remote(
            src.at[rows, pair],
            halo.at[i],
            halo_send.at[i],
            halo_recv.at[i],
            sp=to_next if i < 2 else to_prev,
        )

    share = w_out_ref.shape[0] // nx
    own_part = pl.ds(pl.multiple_of(x * share, share), share)

    def send_cols(i, carry):
        t = lax.rem(tp + i, n_tp)
        remote(
            w_out_ref.at[own_part, cols(t)], wcol.at[tp, own_part], w_sem.at[0], w_sem.at[1], tp=t
        ).start()
        return carry

    def send_stream(i, carry):
        t = lax.rem(tp + i, n_tp)
        remote(stream_ref.at[:, cols(t)], scol.at[tp], st_sem.at[0], st_sem.at[1], tp=t).start()
        return carry

    load(1).wait()
    load(2).wait()
    @pl.when(jnp.logical_not(last))
    def _():
        halo_copy(0).start()
        halo_copy(1).start()

    @pl.when(jnp.logical_not(first))
    def _():
        halo_copy(2).start()
        halo_copy(3).start()
    load(4).wait()
    lax.fori_loop(1, n_tp, send_cols, 0)
    load(5).wait()
    lax.fori_loop(1, n_tp, send_stream, 0)
    wcol[tp, own_part] = w_out_ref[own_part, cols(tp)]
    scol[tp] = stream_ref[:, cols(tp)]
    load(0).wait()
    load(3).wait()
    load(7).wait()
    load(8).wait()

    row_e = lax.broadcasted_iota(jnp.int32, (experts, tok), 0)
    hit_t = jnp.zeros((experts, tok), F32)
    weight_t = jnp.zeros((experts, tok), F32)
    for k in range(topk):
        hit = row_e == routes_ref[k : k + 1, :]
        hit_t = jnp.where(hit, 1.0, hit_t)
        weight_t = jnp.where(hit, rw_ref[k : k + 1, :], weight_t)
    early = lax.broadcasted_iota(jnp.int32, (tok, tok), 0)
    late = lax.broadcasted_iota(jnp.int32, (tok, tok), 1)
    before = (early < late) & (early // rows_dev == late // rows_dev)
    rank_t = dot(hit_t.astype(BF), jnp.where(before, 1.0, 0.0).astype(BF))
    slot_t = jnp.where(hit_t > 0, rank_t, -1.0)
    stab[...] = slot_t
    slot_row = lax.broadcasted_iota(jnp.int32, (slots, tok), 0)
    slot_tok = lax.broadcasted_iota(jnp.int32, (slots, tok), 1)
    in_block = (slot_row // CAP) == (slot_tok // rows_dev)
    slot_rank = jnp.where(in_block, slot_row % CAP, -2).astype(F32)

    def table_rows(e, carry):
        line = stab[pl.ds(e, 1), :]
        ptab[pl.ds(pl.multiple_of(e * slots, slots), slots), :] = jnp.where(
            line == slot_rank, 1.0, 0.0
        ).astype(BF)
        return carry

    lax.fori_loop(0, experts, table_rows, 0)

    @pl.when(first)
    def _():
        halo[0] = jnp.zeros(halo.shape[1:], BF)
        halo[1] = jnp.zeros(halo.shape[1:], BF)

    @pl.when(last)
    def _():
        halo[2] = jnp.zeros(halo.shape[1:], BF)
        halo[3] = jnp.zeros(halo.shape[1:], BF)

    with mark("halo_wait"):
        @pl.when(jnp.logical_not(first))
        def _():
            halo_copy(0).wait_recv()
            halo_copy(1).wait_recv()

        @pl.when(jnp.logical_not(last))
        def _():
            halo_copy(2).wait_recv()
            halo_copy(3).wait_recv()

    odd = head_kv % 2
    query = q_ref[...]
    empty = jnp.zeros_like(query)
    query = jnp.concatenate(
        [jnp.where(odd == 0, query, empty), jnp.where(odd == 0, empty, query)], axis=0
    )
    sink = sink_ref[0:1, 0:1]
    key_i = lax.broadcasted_iota(jnp.int32, (WINDOW, WINDOW), 0)
    query_i = lax.broadcasted_iota(jnp.int32, (WINDOW, WINDOW), 1)
    blocks = tok // WINDOW
    for n in range(blocks):
        q_n = query[:, n * WINDOW : (n + 1) * WINDOW]
        parts = []
        for j in (-1, 0, 1):
            b = n + j
            if b < 0:
                key, value = halo[0], halo[1]
                allowed = (query_i <= key_i) & jnp.logical_not(first)
            elif b == blocks:
                key, value = halo[2], halo[3]
                allowed = (key_i <= query_i) & jnp.logical_not(last)
            else:
                rows = pl.ds(b * WINDOW, WINDOW)
                key, value = k_ref[rows, pair], v_ref[rows, pair]
                allowed = (query_i <= key_i, None, key_i <= query_i)[j + 1]
            score = dot(key, q_n) * (hd**-0.5)
            if allowed is not None:
                score = jnp.where(allowed, score, -jnp.inf)
            parts.append((score, value))
        peak = jnp.maximum(sink, jnp.max(parts[0][0], axis=0, keepdims=True))
        for score, _v in parts[1:]:
            peak = jnp.maximum(peak, jnp.max(score, axis=0, keepdims=True))
        exps = [jnp.exp(score - peak) for score, _v in parts]
        total = jnp.exp(sink - peak)
        for e in exps:
            total = total + jnp.sum(e, axis=0, keepdims=True)
        mix = None
        for e, (_s, value) in zip(exps, parts):
            prob = (e / total).astype(BF)
            term = dot(value, prob, TN)
            mix = term if mix is None else mix + term
        mine = jnp.where(odd == 0, mix[:hd], mix[hd:])
        abuf[tp, :, n * WINDOW : (n + 1) * WINDOW] = mine.astype(BF)

    def peer_of(t):
        return 2 * (t // 2) + 1 - t % 2

    partner = peer_of(tp)

    def to_partner(t):
        return remote(abuf.at[t], abuf.at[t], a_send, a_recv.at[t], tp=partner)

    def to_chip(t, h):
        return remote(abuf.at[t], abuf.at[t], a_send, a_recv.at[t], tp=2 * chip(h) + c)

    for h in range(half, 0, -1):
        to_chip(tp, h).start()
        if h < half:
            to_chip(tp, -h).start()
    to_partner(tp).start()

    def w_along_x(j):
        part = wcol.at[:, own_part]
        to = z * nx + lax.rem(x + j, nx)
        return remote(part, part, wx_send.at[j - 1], wx_recv.at[j - 1], sp=to)

    with mark("w_wait"):
        wait_for(wcol.at[pl.ds(0, n_tp - 1), own_part], w_sem.at[1])
    for j in range(1, nx):
        w_along_x(j).start()

    for i in (6, 9, 10, 12, 13, 11, 14):
        load(i).wait()
    for i in range(d_model // 128):
        some = slice(i * 128, (i + 1) * 128)
        gain = gain_ref[i : i + 1, :].astype(F32)
        for e in range(exp_dev):
            wexp[e, :fh, some] = (w_gate_ref[e, :, some].astype(F32) * gain).astype(BF)
            wexp[e, fh:, some] = (w_up_ref[e, :, some].astype(F32) * gain).astype(BF)
        wexp[exp_dev, :fh, some] = (sg_ref[:, some].astype(F32) * gain).astype(BF)
        wexp[exp_dev, fh:, some] = (su_ref[:, some].astype(F32) * gain).astype(BF)

    with mark("att_wait"):
        for h in range(1, half + 1):
            for sign in (1, -1):
                if h == half and sign == -1:
                    continue
                t = 2 * chip(-sign * h) + c
                wait_for(abuf.at[t], a_recv.at[t])
                to_partner(t).start()

    for e in range(exp_dev):
        wdt[e] = w_down_ref[e].astype(F32).T.astype(BF)
    wdt[exp_dev] = sd_ref[...].astype(F32).T.astype(BF)

    with mark("att_wait2"):
        for j in range(1, nx):
            w_along_x(j).wait_recv()
        wait_for(scol.at[pl.ds(0, n_tp - 1)], st_sem.at[1])
        for i in range(ny):
            t = 2 * chip(i) + 1 - c
            wait_for(abuf.at[t], a_recv.at[t])
    projected = dot(
        abuf[...].reshape(n_tp * hd, tok), wcol[...].reshape(n_tp * hd, dc), TN
    )
    mixed = (scol[...].reshape(tok, dc).astype(F32) + projected).astype(BF)
    resid[...] = mixed
    sbuf[:, cols(tp)] = mixed

    def dest(i, j):
        return lax.rem(z - order[i] + nz, nz) * nx + lax.rem(x + j, nx)

    def source(i, j):
        return lax.rem(z + order[i], nz) * nx + lax.rem(x + j, nx)

    def spot(pos):
        return pl.ds(pl.multiple_of(pos * slots, slots), slots)

    def chunk_rows(k):
        return pl.ds(pl.multiple_of(k * crow, crow), crow)

    def ring_start(block, send, recv, near=0):
        for t in (2 * chip(1) + c, 2 * chip(-1) + c, partner)[2 if near else 0 :]:
            remote(block(tp), block(tp), send, recv(tp), tp=t).start()

    def pass_on(block, send, recv, h, sign, near=0):
        t = 2 * chip(-sign * h) + c
        onto = 2 * chip(sign) + c
        if near <= h < half - 1:
            remote(block(t), block(t), send, recv(t), tp=onto).start()
        elif near <= h == half - 1:

            @pl.when(c == (0 if sign == 1 else 1))
            def _():
                remote(block(t), block(t), send, recv(t), tp=onto).start()

        remote(block(t), block(t), send, recv(t), tp=partner).start()

    def ring_hop(block, send, recv, h, near=0):
        for sign in (1, -1):
            if h < half or sign == 1:
                t = 2 * chip(-sign * h) + c
                wait_for(block(t), recv(t))
                pass_on(block, send, recv, h, sign, near)

    def to_all(block, send, recv):
        for h in range(half, 0, -1):
            for sign in (1, -1):
                if h < half or sign == 1:
                    onto = 2 * chip(sign * h) + c
                    remote(block(tp), block(tp), send, recv(tp), tp=onto).start()
        remote(block(tp), block(tp), send, recv(tp), tp=partner).start()

    def ring_end(block, recv):
        for i in range(ny):
            t = 2 * chip(i) + 1 - c
            wait_for(block(t), recv(t))

    tok_shared = (
        lambda t: sbuf.at[:, cols(t)],
        ts_send,
        lambda t: ts_recv.at[t],
    )
    hid_shared = (
        lambda t: hs.at[units(t), :],
        hs_send,
        lambda t: hs_recv.at[t],
    )

    def tok_ring(k):
        return (
            lambda t: gbuf.at[:, chunk_rows(k), cols(t)],
            t_send.at[k],
            lambda t: t_recv.at[k, t],
        )

    def hid_ring(k):
        return (
            lambda t: hbuf.at[:, units(t), chunk_rows(k)],
            h_send.at[k],
            lambda t: h_recv.at[k, t],
        )

    ring_start(*tok_shared)
    pieces = min(4, n_sp)
    count = n_sp // pieces
    with mark("dispdot"):
        for part in range(pieces):
            size = count * exp_dev * slots
            rows = dot(ptab[part * size : (part + 1) * size, :], mixed)
            obuf[part * count : (part + 1) * count] = rows.astype(BF).reshape(
                count, exp_dev, slots, dc
            )

    def shown(n):
        return 2 * chip((n + 1) // 2 * (-1 if n % 2 else 1)) + c

    def send_rows(n, i):
        for j in range(nx):
            if i == own_chunk and j == 0:
                gbuf[:, spot(i * nx + x), cols(shown(n))] = obuf[n * n_sp + sp]
            else:
                d = dest(i, j)
                remote(
                    obuf.at[n * n_sp + d],
                    gbuf.at[:, spot(i * nx + x), cols(shown(n))],
                    d_send,
                    d_recv.at[i, n],
                    sp=d,
                ).start()

    def beside(h):
        return jnp.concatenate(
            [sbuf[:, cols(shown(2 * h - 1))], sbuf[:, cols(shown(2 * h))]], axis=1
        )

    def make_rows(h, at, blocks, both):
        size = exp_dev * slots
        some = pl.ds(pl.multiple_of(at * size, size), blocks * size)
        rows = dot(ptab[some, :], both)
        for n in (2 * h - 1, 2 * h):
            half_rows = rows[:, :dc] if n % 2 else rows[:, dc:]
            obuf[pl.ds(n * n_sp + at, blocks)] = half_rows.astype(BF).reshape(
                blocks, exp_dev, slots, dc
            )

    def rows_arrived(n, k):
        rows = (nx - (1 if k == own_chunk else 0)) * slots
        if rows:
            wait_for(gbuf.at[:, pl.ds(0, rows), cols(tp)], d_recv.at[k, n])

    def inject(h):
        both = beside(h)
        takers = [i for i in range(n_chunk) if near[i] >= h]
        if 2 * len(takers) > n_chunk:
            for part in range(pieces):
                make_rows(h, part * count, count, both)
        else:
            for i in takers:
                make_rows(h, lax.rem(z - order[i] + nz, nz) * nx, nx, both)
        for i in range(n_chunk):
            if h == 1 and i >= ahead:
                send_rows(0, i)
            if near[i] >= h:
                send_rows(2 * h - 1, i)
                send_rows(2 * h, i)

    ahead = min(4, n_chunk)
    for i in range(ahead):
        send_rows(0, i)

    slot_c = slot_t.T.astype(BF)
    weight_c = weight_t.T.astype(BF)
    width = min(512, experts * slots)
    for part in range(experts * slots // width):
        m = lax.broadcasted_iota(jnp.int32, (experts, width), 1) + part * width
        e_i = lax.broadcasted_iota(jnp.int32, (experts, width), 0)
        spread = jnp.where(m // slots == e_i, 1.0, 0.0).astype(BF)
        m2 = lax.broadcasted_iota(jnp.int32, (tok, width), 1) + part * width
        r2 = lax.broadcasted_iota(jnp.int32, (tok, width), 0)
        want = jnp.where((m2 % slots) // CAP == r2 // rows_dev, m2 % CAP, -2).astype(F32)
        table = jnp.where(dot(slot_c, spread) == want, dot(weight_c, spread), 0.0)
        ctab[:, part * width : (part + 1) * width] = table.astype(BF)

    def hidden_of(rows, e):
        wide = rows.astype(F32)
        squares = wide * wide
        part = squares[:, :128]
        for i in range(1, d_model // 128):
            part = part + squares[:, i * 128 : (i + 1) * 128]
        total = jnp.sum(part.T, axis=0, keepdims=True)
        scale = lax.rsqrt(total / d_model + NORM_EPS)
        acts = dot(wexp[e], rows, NT) * scale
        gate, up = acts[:fh], acts[fh:]
        return (gate / (1.0 + jnp.exp(-gate)) * up).astype(BF)

    def up_shared():
        ring_end(tok_shared[0], tok_shared[2])
        hs[units(tp), :] = hidden_of(sbuf[...], exp_dev)
        ring_start(*hid_shared)

    def up_chunk(k):
        ring_end(tok_ring(k)[0], tok_ring(k)[2])
        for e in range(exp_dev):
            hbuf[e, units(tp), chunk_rows(k)] = hidden_of(gbuf[e, chunk_rows(k), :], e)
        if not direct[k]:
            ring_start(*hid_ring(k))

    def down_shared():
        ring_end(hid_shared[0], hid_shared[2])
        shared_out[...] = dot(wdt[exp_dev], hs[...]).T

    def down_chunk(k):
        ring_end(hid_ring(k)[0], hid_ring(k)[2])
        for e in range(exp_dev):
            res = dot(wdt[e], hbuf[e, :, chunk_rows(k)])
            ybuf[e, chunk_rows(k), :] = res.T.astype(BF)
        return_chunk(k)

    def give_back(i, j):
        s = source(i, j)
        pos = i * nx + lax.rem(x + j, nx)
        return remote(ybuf.at[:, spot(pos), :], rbuf.at[sp], r_send, r_recv, sp=s)

    def return_chunk(k):
        for j in range(nx):
            if k == own_chunk and j == 0:
                rbuf[sp] = ybuf[:, spot(k * nx + x), :]
            else:
                give_back(k, j).start()

    def tok_in(k):
        rows_arrived(0, k)
        ring_start(*tok_ring(k), near[k])
        for h in range(1, near[k] + 1):
            for n, sign in ((2 * h - 1, 1), (2 * h, -1)):
                rows_arrived(n, k)
                pass_on(*tok_ring(k), h, sign, near[k])

    slots_of = collections.defaultdict(list)
    for h in range(1, half + 1):
        slots_of[h - 2].append((2, f"tokS_{h}", lambda h=h: ring_hop(*tok_shared, h)))
        slots_of[half - 2 + h].append((1, f"hidS_{h}", lambda h=h: ring_hop(*hid_shared, h)))
    slots_of[half - 2].append((3, "upS", up_shared))
    slots_of[2 * half - 2].append((4, "downS", down_shared))
    for h in range(1, max(half, 2)):
        slots_of[h - 2].append((3, f"inject{h}", lambda h=h: inject(h)))
    for k in range(n_chunk):
        full_at = k + half - 1 - (k == n_chunk - 1)
        slots_of[full_at - half + near[k]].append((2, f"in{k}", lambda k=k: tok_in(k)))
        for h in range(near[k] + 1, half + 1):
            slots_of[full_at - half + h].append(
                (2, f"tok{k}_{h}", lambda k=k, h=h: ring_hop(*tok_ring(k), h))
            )
        up_at = full_at + 1
        slots_of[up_at].append((1.5, f"up{k}", lambda k=k: up_chunk(k)))
        if direct[k]:
            slots_of[up_at + 1].append((1.5, f"hid{k}", lambda k=k: to_all(*hid_ring(k))))
        for h in range(1, half + 1):
            slots_of[up_at + (half if direct[k] else h)].append(
                (1, f"hid{k}_{h}", lambda k=k, h=h: ring_hop(*hid_ring(k), h, direct[k]))
            )
        slots_of[up_at + half].append((4, f"down{k}", lambda k=k: down_chunk(k)))
    for slot in sorted(slots_of):
        for _r, name, step in sorted(slots_of[slot], key=lambda item: item[0]):
            with mark(name):
                step()

    wait_for(wcol.at[pl.ds(0, n_tp - 1), own_part], w_sem.at[0])
    for j in range(1, nx):
        w_along_x(j).wait_send()
    wait_for(scol.at[pl.ds(0, n_tp - 1)], st_sem.at[0])

    @pl.when(jnp.logical_not(last))
    def _():
        halo_copy(0).wait_send()
        halo_copy(1).wait_send()

    @pl.when(jnp.logical_not(first))
    def _():
        halo_copy(2).wait_send()
        halo_copy(3).wait_send()

    wait_for(abuf.at[pl.ds(0, n_tp - 1)], a_send)
    count = sum((1 + 2 * near[i]) * (nx - (i == own_chunk)) for i in range(n_chunk))
    wait_for(obuf.at[pl.ds(0, count)], d_send)
    wait_for(sbuf.at[:, pl.ds(0, (n_tp - 1) * dc)], ts_send)
    wait_for(hs.at[pl.ds(0, (n_tp - 1) * fh), :], hs_send)
    for k in range(n_chunk):
        wait_for(
            gbuf.at[:, chunk_rows(k), pl.ds(0, (n_tp - 1 - 2 * near[k]) * dc)], t_send.at[k]
        )
        wait_for(hbuf.at[:, pl.ds(0, (n_tp - 1) * fh), chunk_rows(k)], h_send.at[k])
    wait_for(rbuf.at[pl.ds(0, n_sp - 1)], r_send)

    with mark("ret_wait"):
        wait_for(rbuf.at[pl.ds(0, n_sp - 1)], r_recv)
    with mark("combine"):
        routed = dot(ctab[...], rbuf[...].reshape(experts * slots, dc))
        out_ref[...] = (resid[...].astype(F32) + routed + shared_out[...]).astype(BF)


def local(
    queries,
    keys,
    values,
    sink,
    w_out,
    stream,
    gain,
    routes,
    route_weights,
    w_gate,
    w_up,
    w_down,
    shared_gate,
    shared_up,
    shared_down,
    *,
    kv_group,
    order,
    near,
    nx,
):
    n_tp = lax.axis_size("tp")
    n_sp = lax.axis_size("sp")
    tok = queries.shape[0]
    rows, d_model = stream.shape
    dc = d_model // n_tp
    exp_dev, fh, _ = w_gate.shape
    experts = exp_dev * n_sp
    slots = n_tp * CAP
    n_rows = n_sp * slots
    n_chunk = len(order)
    vm = pltpu.VMEM
    dma = pltpu.SemaphoreType.DMA
    inputs = (
        queries.T,
        keys,
        values,
        sink.reshape(1, 1),
        w_out,
        stream,
        gain.reshape(d_model // 128, 128),
        routes.T,
        route_weights.T,
        w_gate,
        w_up,
        w_down,
        shared_gate,
        shared_up,
        shared_down,
    )
    return pl.pallas_call(
        functools.partial(kernel, kv_group=kv_group, order=order, near=near, nx=nx),
        out_shape=jax.ShapeDtypeStruct((tok, dc), BF),
        in_specs=[pl.BlockSpec(memory_space=pl.ANY)] * 15,
        out_specs=pl.BlockSpec(memory_space=vm),
        scratch_shapes=[
            *[vm(a.shape, a.dtype) for a in inputs],
            dma((len(inputs),)),
            vm((n_tp, w_out.shape[0], dc), BF),
            vm((n_tp, rows, dc), BF),
            vm((4, WINDOW, 2 * HD), BF),
            vm((n_tp, HD, tok), BF),
            vm((tok, d_model), BF),
            vm((exp_dev, n_rows, d_model), BF),
            vm(((1 + 2 * max(near)) * n_sp, exp_dev, slots, dc), BF),
            vm((n_tp * fh, tok), BF),
            vm((exp_dev, n_tp * fh, n_rows), BF),
            vm((exp_dev, n_rows, dc), BF),
            vm((n_sp, exp_dev, slots, dc), BF),
            vm((experts * slots, tok), BF),
            vm((tok, experts * slots), BF),
            vm((experts, tok), F32),
            vm((exp_dev + 1, 2 * fh, d_model), BF),
            vm((exp_dev + 1, dc, n_tp * fh), BF),
            vm((tok, dc), BF),
            vm((tok, dc), F32),
            dma((2,)),
            dma((max(nx - 1, 1),)),
            dma((max(nx - 1, 1),)),
            dma((2,)),
            dma((4,)),
            dma((4,)),
            dma(()),
            dma((n_tp,)),
            dma(()),
            dma((n_chunk, 1 + 2 * max(near))),
            dma(()),
            dma(()),
            dma(()),
            dma((n_tp,)),
            dma((n_chunk,)),
            dma((n_chunk, n_tp)),
            dma(()),
            dma((n_tp,)),
            dma((n_chunk,)),
            dma((n_chunk, n_tp)),
        ],
        compiler_params=pltpu.CompilerParams(
            collective_id=0, has_side_effects=True, vmem_limit_bytes=60 * 1024 * 1024
        ),
    )(*inputs)


def solution(mesh, kv_group=4, order=Z_ORDER, near=NEAR, nx=NX):
    placed = (
        P("sp", "tp"),
        P("sp", None),
        P("sp", None),
        P("tp"),
        P("tp", None),
        P(("sp", "tp"), None),
        P(),
        P("sp", None),
        P("sp", None),
        P("sp", "tp", None),
        P("sp", "tp", None),
        P("sp", None, "tp"),
        P("tp", None),
        P("tp", None),
        P(None, "tp"),
    )
    return jax.shard_map(
        functools.partial(local, kv_group=kv_group, order=order, near=near, nx=nx),
        mesh=mesh,
        in_specs=placed,
        out_specs=P("sp", "tp"),
        check_vma=False,
    )
```

```python
import collections
import contextlib
import functools

import jax
import jax.numpy as jnp
from jax import lax
from jax.experimental import pallas as pl
from jax.experimental.pallas import tpu as pltpu
from jax.sharding import PartitionSpec as P

HD = 64
WINDOW = 128
CAP = 2
NX = 4
NEAR = (0, 0, 0, 0, 3, 1, 3, 3)
FULL = (3, 4, 5, 6, 6, 7, 7, 8)
DIRECT = 0
Z_ORDER = (1, 6, 3, 4, 0, 5, 2, 7)
NORM_EPS = 1e-05
mark = contextlib.nullcontext
BF = jnp.bfloat16
F32 = jnp.float32

NT = (((1,), (1,)), ((), ()))
TN = (((0,), (0,)), ((), ()))


def dot(a, b, dims=(((1,), (0,)), ((), ()))):
    return lax.dot_general(a, b, dims, preferred_element_type=F32)


def kernel(
    q_in,
    k_in,
    v_in,
    sink_in,
    w_out_in,
    stream_in,
    gain_in,
    routes_in,
    rw_in,
    w_gate_in,
    w_up_in,
    w_down_in,
    sg_in,
    su_in,
    sd_in,
    out_ref,
    q_ref,
    k_ref,
    v_ref,
    sink_ref,
    w_out_ref,
    stream_ref,
    gain_ref,
    routes_ref,
    rw_ref,
    w_gate_ref,
    w_up_ref,
    w_down_ref,
    sg_ref,
    su_ref,
    sd_ref,
    in_sem,
    wcol,
    scol,
    halo,
    abuf,
    sbuf,
    gbuf,
    obuf,
    hs,
    hbuf,
    ybuf,
    rbuf,
    ptab,
    ctab,
    stab,
    wexp,
    wdt,
    resid,
    shared_out,
    w_sem,
    wx_send,
    wx_recv,
    st_sem,
    halo_send,
    halo_recv,
    a_send,
    a_recv,
    d_send,
    d_recv,
    r_send,
    r_recv,
    ts_send,
    ts_recv,
    t_send,
    t_recv,
    hs_send,
    hs_recv,
    h_send,
    h_recv,
    *,
    kv_group,
    order,
    near,
    nx,
):
    hd, tok = q_ref.shape
    d_model = stream_ref.shape[1]
    rows_dev = stream_ref.shape[0]
    n_tp = lax.axis_size("tp")
    n_sp = lax.axis_size("sp")
    ny = n_tp // 2
    nz = n_sp // nx
    dc = d_model // n_tp
    exp_dev, fh = w_gate_ref.shape[0], w_gate_ref.shape[1]
    experts = exp_dev * n_sp
    topk = routes_ref.shape[0]
    slots = n_tp * CAP
    n_chunk = len(order)
    own_chunk = order.index(0)
    direct = [ny // 2 if k >= n_chunk - DIRECT else 0 for k in range(n_chunk)]
    crow = nx * slots
    sp = lax.axis_index("sp")
    tp = lax.axis_index("tp")
    y, c = tp // 2, tp % 2
    z, x = sp // nx, sp % nx
    half = ny // 2

    def cols(t):
        return pl.ds(pl.multiple_of(t * dc, dc), dc)

    def units(t):
        return pl.ds(pl.multiple_of(t * fh, fh), fh)

    def chip(dy):
        return lax.rem(y + dy + ny, ny)

    def remote(src, dst, send, recv, **device):
        return pltpu.make_async_remote_copy(
            src_ref=src,
            dst_ref=dst,
            send_sem=send,
            recv_sem=recv,
            device_id=device,
            device_id_type=pl.DeviceIdType.MESH,
        )

    def wait_for(ref, sem):
        pltpu.make_async_copy(ref, ref, sem).wait()

    pairs = (
        (q_in, q_ref),
        (k_in, k_ref),
        (v_in, v_ref),
        (sink_in, sink_ref),
        (w_out_in, w_out_ref),
        (stream_in, stream_ref),
        (gain_in, gain_ref),
        (routes_in, routes_ref),
        (rw_in, rw_ref),
        (w_gate_in, w_gate_ref),
        (w_up_in, w_up_ref),
        (w_down_in, w_down_ref),
        (sg_in, sg_ref),
        (su_in, su_ref),
        (sd_in, sd_ref),
    )

    def load(i):
        return pltpu.make_async_copy(pairs[i][0], pairs[i][1], in_sem.at[i])

    barrier = pltpu.get_barrier_semaphore()

    def greet_tp(i, carry):
        pl.semaphore_signal(barrier, inc=1, device_id={"tp": lax.rem(tp + i, n_tp)})
        return carry

    def greet_sp(i, carry):
        pl.semaphore_signal(barrier, inc=1, device_id={"sp": lax.rem(sp + i, n_sp)})
        return carry

    lax.fori_loop(1, n_tp, greet_tp, 0)
    lax.fori_loop(1, n_sp, greet_sp, 0)
    for i in (1, 2, 4, 5, 0, 3, 7, 8, 6, 9, 10, 12, 13, 11, 14):
        load(i).start()

    with mark("barrier"):
        pl.semaphore_wait(barrier, n_tp - 1 + n_sp - 1)

    head_kv = tp // kv_group
    pair = pl.ds(pl.multiple_of((head_kv // 2) * 2 * hd, 2 * hd), 2 * hd)
    last, first = sp == n_sp - 1, sp == 0
    to_next = lax.rem(sp + 1, n_sp)
    to_prev = lax.rem(sp + n_sp - 1, n_sp)

    def halo_copy(i):
        src = (k_ref, v_ref)[i % 2]
        rows = pl.ds(tok - WINDOW, WINDOW) if i < 2 else pl.ds(0, WINDOW)
        return remote(
            src.at[rows, pair],
            halo.at[i],
            halo_send.at[i],
            halo_recv.at[i],
            sp=to_next if i < 2 else to_prev,
        )

    share = w_out_ref.shape[0] // nx
    own_part = pl.ds(pl.multiple_of(x * share, share), share)

    def send_cols(i, carry):
        t = lax.rem(tp + i, n_tp)
        remote(
            w_out_ref.at[own_part, cols(t)], wcol.at[tp, own_part], w_sem.at[0], w_sem.at[1], tp=t
        ).start()
        return carry

    def send_stream(i, carry):
        t = lax.rem(tp + i, n_tp)
        remote(stream_ref.at[:, cols(t)], scol.at[tp], st_sem.at[0], st_sem.at[1], tp=t).start()
        return carry

    load(1).wait()
    load(2).wait()
    @pl.when(jnp.logical_not(last))
    def _():
        halo_copy(0).start()
        halo_copy(1).start()

    @pl.when(jnp.logical_not(first))
    def _():
        halo_copy(2).start()
        halo_copy(3).start()
    load(4).wait()
    lax.fori_loop(1, n_tp, send_cols, 0)
    load(5).wait()
    lax.fori_loop(1, n_tp, send_stream, 0)
    wcol[tp, own_part] = w_out_ref[own_part, cols(tp)]
    scol[tp] = stream_ref[:, cols(tp)]
    load(0).wait()
    load(3).wait()
    load(7).wait()
    load(8).wait()

    row_e = lax.broadcasted_iota(jnp.int32, (experts, tok), 0)
    hit_t = jnp.zeros((experts, tok), F32)
    weight_t = jnp.zeros((experts, tok), F32)
    for k in range(topk):
        hit = row_e == routes_ref[k : k + 1, :]
        hit_t = jnp.where(hit, 1.0, hit_t)
        weight_t = jnp.where(hit, rw_ref[k : k + 1, :], weight_t)
    early = lax.broadcasted_iota(jnp.int32, (tok, tok), 0)
    late = lax.broadcasted_iota(jnp.int32, (tok, tok), 1)
    before = (early < late) & (early // rows_dev == late // rows_dev)
    rank_t = dot(hit_t.astype(BF), jnp.where(before, 1.0, 0.0).astype(BF))
    slot_t = jnp.where(hit_t > 0, rank_t, -1.0)
    stab[...] = slot_t
    slot_row = lax.broadcasted_iota(jnp.int32, (slots, tok), 0)
    slot_tok = lax.broadcasted_iota(jnp.int32, (slots, tok), 1)
    in_block = (slot_row // CAP) == (slot_tok // rows_dev)
    slot_rank = jnp.where(in_block, slot_row % CAP, -2).astype(F32)

    def table_rows(e, carry):
        line = stab[pl.ds(e, 1), :]
        ptab[pl.ds(pl.multiple_of(e * slots, slots), slots), :] = jnp.where(
            line == slot_rank, 1.0, 0.0
        ).astype(BF)
        return carry

    lax.fori_loop(0, experts, table_rows, 0)

    @pl.when(first)
    def _():
        halo[0] = jnp.zeros(halo.shape[1:], BF)
        halo[1] = jnp.zeros(halo.shape[1:], BF)

    @pl.when(last)
    def _():
        halo[2] = jnp.zeros(halo.shape[1:], BF)
        halo[3] = jnp.zeros(halo.shape[1:], BF)

    with mark("halo_wait"):
        @pl.when(jnp.logical_not(first))
        def _():
            halo_copy(0).wait_recv()
            halo_copy(1).wait_recv()

        @pl.when(jnp.logical_not(last))
        def _():
            halo_copy(2).wait_recv()
            halo_copy(3).wait_recv()

    odd = head_kv % 2
    query = q_ref[...]
    empty = jnp.zeros_like(query)
    query = jnp.concatenate(
        [jnp.where(odd == 0, query, empty), jnp.where(odd == 0, empty, query)], axis=0
    )
    sink = sink_ref[0:1, 0:1]
    key_i = lax.broadcasted_iota(jnp.int32, (WINDOW, WINDOW), 0)
    query_i = lax.broadcasted_iota(jnp.int32, (WINDOW, WINDOW), 1)
    blocks = tok // WINDOW
    for n in range(blocks):
        q_n = query[:, n * WINDOW : (n + 1) * WINDOW]
        parts = []
        for j in (-1, 0, 1):
            b = n + j
            if b < 0:
                key, value = halo[0], halo[1]
                allowed = (query_i <= key_i) & jnp.logical_not(first)
            elif b == blocks:
                key, value = halo[2], halo[3]
                allowed = (key_i <= query_i) & jnp.logical_not(last)
            else:
                rows = pl.ds(b * WINDOW, WINDOW)
                key, value = k_ref[rows, pair], v_ref[rows, pair]
                allowed = (query_i <= key_i, None, key_i <= query_i)[j + 1]
            score = dot(key, q_n) * (hd**-0.5)
            if allowed is not None:
                score = jnp.where(allowed, score, -jnp.inf)
            parts.append((score, value))
        peak = jnp.maximum(sink, jnp.max(parts[0][0], axis=0, keepdims=True))
        for score, _v in parts[1:]:
            peak = jnp.maximum(peak, jnp.max(score, axis=0, keepdims=True))
        exps = [jnp.exp(score - peak) for score, _v in parts]
        total = jnp.exp(sink - peak)
        for e in exps:
            total = total + jnp.sum(e, axis=0, keepdims=True)
        mix = None
        for e, (_s, value) in zip(exps, parts):
            prob = (e / total).astype(BF)
            term = dot(value, prob, TN)
            mix = term if mix is None else mix + term
        mine = jnp.where(odd == 0, mix[:hd], mix[hd:])
        abuf[tp, :, n * WINDOW : (n + 1) * WINDOW] = mine.astype(BF)

    def peer_of(t):
        return 2 * (t // 2) + 1 - t % 2

    partner = peer_of(tp)

    def to_partner(t):
        return remote(abuf.at[t], abuf.at[t], a_send, a_recv.at[t], tp=partner)

    def to_chip(t, h):
        return remote(abuf.at[t], abuf.at[t], a_send, a_recv.at[t], tp=2 * chip(h) + c)

    for h in range(half, 0, -1):
        to_chip(tp, h).start()
        if h < half:
            to_chip(tp, -h).start()
    to_partner(tp).start()

    def w_along_x(j):
        part = wcol.at[:, own_part]
        to = z * nx + lax.rem(x + j, nx)
        return remote(part, part, wx_send.at[j - 1], wx_recv.at[j - 1], sp=to)

    with mark("w_wait"):
        wait_for(wcol.at[pl.ds(0, n_tp - 1), own_part], w_sem.at[1])
    for j in range(1, nx):
        w_along_x(j).start()

    for i in (6, 9, 10, 12, 13, 11, 14):
        load(i).wait()
    for i in range(d_model // 128):
        some = slice(i * 128, (i + 1) * 128)
        gain = gain_ref[i : i + 1, :].astype(F32)
        for e in range(exp_dev):
            wexp[e, :fh, some] = (w_gate_ref[e, :, some].astype(F32) * gain).astype(BF)
            wexp[e, fh:, some] = (w_up_ref[e, :, some].astype(F32) * gain).astype(BF)
        wexp[exp_dev, :fh, some] = (sg_ref[:, some].astype(F32) * gain).astype(BF)
        wexp[exp_dev, fh:, some] = (su_ref[:, some].astype(F32) * gain).astype(BF)

    with mark("att_wait"):
        for h in range(1, half + 1):
            for sign in (1, -1):
                if h == half and sign == -1:
                    continue
                t = 2 * chip(-sign * h) + c
                wait_for(abuf.at[t], a_recv.at[t])
                to_partner(t).start()

    for e in range(exp_dev):
        wdt[e] = w_down_ref[e].astype(F32).T.astype(BF)
    wdt[exp_dev] = sd_ref[...].astype(F32).T.astype(BF)

    with mark("att_wait2"):
        for j in range(1, nx):
            w_along_x(j).wait_recv()
        wait_for(scol.at[pl.ds(0, n_tp - 1)], st_sem.at[1])
        for i in range(ny):
            t = 2 * chip(i) + 1 - c
            wait_for(abuf.at[t], a_recv.at[t])
    projected = dot(
        abuf[...].reshape(n_tp * hd, tok), wcol[...].reshape(n_tp * hd, dc), TN
    )
    mixed = (scol[...].reshape(tok, dc).astype(F32) + projected).astype(BF)
    resid[...] = mixed
    sbuf[:, cols(tp)] = mixed

    def dest(i, j):
        return lax.rem(z - order[i] + nz, nz) * nx + lax.rem(x + j, nx)

    def source(i, j):
        return lax.rem(z + order[i], nz) * nx + lax.rem(x + j, nx)

    def spot(pos):
        return pl.ds(pl.multiple_of(pos * slots, slots), slots)

    def chunk_rows(k):
        return pl.ds(pl.multiple_of(k * crow, crow), crow)

    def ring_start(block, send, recv, near=0):
        for t in (2 * chip(1) + c, 2 * chip(-1) + c, partner)[2 if near else 0 :]:
            remote(block(tp), block(tp), send, recv(tp), tp=t).start()

    def pass_on(block, send, recv, h, sign, near=0):
        t = 2 * chip(-sign * h) + c
        onto = 2 * chip(sign) + c
        if near <= h < half - 1:
            remote(block(t), block(t), send, recv(t), tp=onto).start()
        elif near <= h == half - 1:

            @pl.when(c == (0 if sign == 1 else 1))
            def _():
                remote(block(t), block(t), send, recv(t), tp=onto).start()

        remote(block(t), block(t), send, recv(t), tp=partner).start()

    def ring_hop(block, send, recv, h, near=0):
        for sign in (1, -1):
            if h < half or sign == 1:
                t = 2 * chip(-sign * h) + c
                wait_for(block(t), recv(t))
                pass_on(block, send, recv, h, sign, near)

    def to_all(block, send, recv):
        for h in range(half, 0, -1):
            for sign in (1, -1):
                if h < half or sign == 1:
                    onto = 2 * chip(sign * h) + c
                    remote(block(tp), block(tp), send, recv(tp), tp=onto).start()
        remote(block(tp), block(tp), send, recv(tp), tp=partner).start()

    def ring_end(block, recv):
        for i in range(ny):
            t = 2 * chip(i) + 1 - c
            wait_for(block(t), recv(t))

    tok_shared = (
        lambda t: sbuf.at[:, cols(t)],
        ts_send,
        lambda t: ts_recv.at[t],
    )
    hid_shared = (
        lambda t: hs.at[units(t), :],
        hs_send,
        lambda t: hs_recv.at[t],
    )

    def tok_ring(k):
        return (
            lambda t: gbuf.at[:, chunk_rows(k), cols(t)],
            t_send.at[k],
            lambda t: t_recv.at[k, t],
        )

    def hid_ring(k):
        return (
            lambda t: hbuf.at[:, units(t), chunk_rows(k)],
            h_send.at[k],
            lambda t: h_recv.at[k, t],
        )

    ring_start(*tok_shared)
    pieces = min(4, n_sp)
    count = n_sp // pieces
    with mark("dispdot"):
        for part in range(pieces):
            size = count * exp_dev * slots
            rows = dot(ptab[part * size : (part + 1) * size, :], mixed)
            obuf[part * count : (part + 1) * count] = rows.astype(BF).reshape(
                count, exp_dev, slots, dc
            )

    def shown(n):
        return 2 * chip((n + 1) // 2 * (-1 if n % 2 else 1)) + c

    def send_rows(n, i):
        for j in range(nx):
            if i == own_chunk and j == 0:
                gbuf[:, spot(i * nx + x), cols(shown(n))] = obuf[n * n_sp + sp]
            else:
                d = dest(i, j)
                remote(
                    obuf.at[n * n_sp + d],
                    gbuf.at[:, spot(i * nx + x), cols(shown(n))],
                    d_send,
                    d_recv.at[i, n],
                    sp=d,
                ).start()

    def beside(h):
        return jnp.concatenate(
            [sbuf[:, cols(shown(2 * h - 1))], sbuf[:, cols(shown(2 * h))]], axis=1
        )

    def make_rows(h, at, blocks, both):
        size = exp_dev * slots
        some = pl.ds(pl.multiple_of(at * size, size), blocks * size)
        rows = dot(ptab[some, :], both)
        for n in (2 * h - 1, 2 * h):
            half_rows = rows[:, :dc] if n % 2 else rows[:, dc:]
            obuf[pl.ds(n * n_sp + at, blocks)] = half_rows.astype(BF).reshape(
                blocks, exp_dev, slots, dc
            )

    def rows_arrived(n, k):
        rows = (nx - (1 if k == own_chunk else 0)) * slots
        if rows:
            wait_for(gbuf.at[:, pl.ds(0, rows), cols(tp)], d_recv.at[k, n])

    def inject(h):
        both = beside(h)
        takers = [i for i in range(n_chunk) if near[i] >= h]
        if 2 * len(takers) > n_chunk:
            for part in range(pieces):
                make_rows(h, part * count, count, both)
        else:
            for i in takers:
                make_rows(h, lax.rem(z - order[i] + nz, nz) * nx, nx, both)
        for i in range(n_chunk):
            if h == 1 and i >= ahead:
                send_rows(0, i)
            if near[i] >= h:
                send_rows(2 * h - 1, i)
                send_rows(2 * h, i)

    ahead = min(5, n_chunk)
    for i in range(ahead):
        send_rows(0, i)

    slot_c = slot_t.T.astype(BF)
    weight_c = weight_t.T.astype(BF)
    width = min(512, experts * slots)
    for part in range(experts * slots // width):
        m = lax.broadcasted_iota(jnp.int32, (experts, width), 1) + part * width
        e_i = lax.broadcasted_iota(jnp.int32, (experts, width), 0)
        spread = jnp.where(m // slots == e_i, 1.0, 0.0).astype(BF)
        m2 = lax.broadcasted_iota(jnp.int32, (tok, width), 1) + part * width
        r2 = lax.broadcasted_iota(jnp.int32, (tok, width), 0)
        want = jnp.where((m2 % slots) // CAP == r2 // rows_dev, m2 % CAP, -2).astype(F32)
        table = jnp.where(dot(slot_c, spread) == want, dot(weight_c, spread), 0.0)
        ctab[:, part * width : (part + 1) * width] = table.astype(BF)

    def hidden_of(rows, e):
        wide = rows.astype(F32)
        squares = wide * wide
        part = squares[:, :128]
        for i in range(1, d_model // 128):
            part = part + squares[:, i * 128 : (i + 1) * 128]
        total = jnp.sum(part.T, axis=0, keepdims=True)
        scale = lax.rsqrt(total / d_model + NORM_EPS)
        acts = dot(wexp[e], rows, NT) * scale
        gate, up = acts[:fh], acts[fh:]
        return (gate / (1.0 + jnp.exp(-gate)) * up).astype(BF)

    def up_shared():
        ring_end(tok_shared[0], tok_shared[2])
        hs[units(tp), :] = hidden_of(sbuf[...], exp_dev)
        ring_start(*hid_shared)

    def up_chunk(k):
        ring_end(tok_ring(k)[0], tok_ring(k)[2])
        for e in range(exp_dev):
            hbuf[e, units(tp), chunk_rows(k)] = hidden_of(gbuf[e, chunk_rows(k), :], e)
        if not direct[k]:
            ring_start(*hid_ring(k))

    def down_shared():
        ring_end(hid_shared[0], hid_shared[2])
        shared_out[...] = dot(wdt[exp_dev], hs[...]).T

    def down_chunk(k):
        ring_end(hid_ring(k)[0], hid_ring(k)[2])
        for e in range(exp_dev):
            res = dot(wdt[e], hbuf[e, :, chunk_rows(k)])
            ybuf[e, chunk_rows(k), :] = res.T.astype(BF)
        return_chunk(k)

    def give_back(i, j):
        s = source(i, j)
        pos = i * nx + lax.rem(x + j, nx)
        return remote(ybuf.at[:, spot(pos), :], rbuf.at[sp], r_send, r_recv, sp=s)

    def return_chunk(k):
        for j in range(nx):
            if k == own_chunk and j == 0:
                rbuf[sp] = ybuf[:, spot(k * nx + x), :]
            else:
                give_back(k, j).start()

    def tok_in(k):
        rows_arrived(0, k)
        ring_start(*tok_ring(k), near[k])
        for h in range(1, near[k] + 1):
            for n, sign in ((2 * h - 1, 1), (2 * h, -1)):
                rows_arrived(n, k)
                pass_on(*tok_ring(k), h, sign, near[k])

    slots_of = collections.defaultdict(list)
    for h in range(1, half + 1):
        slots_of[h - 2].append((2, f"tokS_{h}", lambda h=h: ring_hop(*tok_shared, h)))
        slots_of[half - 1 + h].append((2.9, f"hidS_{h}", lambda h=h: ring_hop(*hid_shared, h)))
    slots_of[half - 1].append((1.5, "upS", up_shared))
    slots_of[2 * half + 1].append((1.6, "downS", down_shared))
    for h in range(1, max(half, 2)):
        slots_of[h - 2].append((2 if h == 1 else 3, f"inject{h}", lambda h=h: inject(h)))
    for k in range(n_chunk):
        full_at = FULL[k] + half - 4
        slots_of[full_at - half + near[k]].append((2, f"in{k}", lambda k=k: tok_in(k)))
        for h in range(near[k] + 1, half + 1):
            slots_of[full_at - half + h].append(
                (2, f"tok{k}_{h}", lambda k=k, h=h: ring_hop(*tok_ring(k), h))
            )
        up_at = full_at + 1
        slots_of[up_at].append((1.5, f"up{k}", lambda k=k: up_chunk(k)))
        if direct[k]:
            slots_of[up_at + 1].append((1.5, f"hid{k}", lambda k=k: to_all(*hid_ring(k))))
        for h in range(1, half + 1):
            slots_of[up_at + (half if direct[k] else h)].append(
                (1, f"hid{k}_{h}", lambda k=k, h=h: ring_hop(*hid_ring(k), h, direct[k]))
            )
        slots_of[up_at + half].append((4, f"down{k}", lambda k=k: down_chunk(k)))
    for slot in sorted(slots_of):
        for _r, name, step in sorted(slots_of[slot], key=lambda item: item[0]):
            with mark(name):
                step()

    wait_for(wcol.at[pl.ds(0, n_tp - 1), own_part], w_sem.at[0])
    for j in range(1, nx):
        w_along_x(j).wait_send()
    wait_for(scol.at[pl.ds(0, n_tp - 1)], st_sem.at[0])

    @pl.when(jnp.logical_not(last))
    def _():
        halo_copy(0).wait_send()
        halo_copy(1).wait_send()

    @pl.when(jnp.logical_not(first))
    def _():
        halo_copy(2).wait_send()
        halo_copy(3).wait_send()

    wait_for(abuf.at[pl.ds(0, n_tp - 1)], a_send)
    count = sum((1 + 2 * near[i]) * (nx - (i == own_chunk)) for i in range(n_chunk))
    wait_for(obuf.at[pl.ds(0, count)], d_send)
    wait_for(sbuf.at[:, pl.ds(0, (n_tp - 1) * dc)], ts_send)
    wait_for(hs.at[pl.ds(0, (n_tp - 1) * fh), :], hs_send)
    for k in range(n_chunk):
        wait_for(
            gbuf.at[:, chunk_rows(k), pl.ds(0, (n_tp - 1 - 2 * near[k]) * dc)], t_send.at[k]
        )
        wait_for(hbuf.at[:, pl.ds(0, (n_tp - 1) * fh), chunk_rows(k)], h_send.at[k])
    wait_for(rbuf.at[pl.ds(0, n_sp - 1)], r_send)

    with mark("ret_wait"):
        wait_for(rbuf.at[pl.ds(0, n_sp - 1)], r_recv)
    with mark("combine"):
        routed = dot(ctab[...], rbuf[...].reshape(experts * slots, dc))
        out_ref[...] = (resid[...].astype(F32) + routed + shared_out[...]).astype(BF)


def local(
    queries,
    keys,
    values,
    sink,
    w_out,
    stream,
    gain,
    routes,
    route_weights,
    w_gate,
    w_up,
    w_down,
    shared_gate,
    shared_up,
    shared_down,
    *,
    kv_group,
    order,
    near,
    nx,
):
    n_tp = lax.axis_size("tp")
    n_sp = lax.axis_size("sp")
    tok = queries.shape[0]
    rows, d_model = stream.shape
    dc = d_model // n_tp
    exp_dev, fh, _ = w_gate.shape
    experts = exp_dev * n_sp
    slots = n_tp * CAP
    n_rows = n_sp * slots
    n_chunk = len(order)
    vm = pltpu.VMEM
    dma = pltpu.SemaphoreType.DMA
    inputs = (
        queries.T,
        keys,
        values,
        sink.reshape(1, 1),
        w_out,
        stream,
        gain.reshape(d_model // 128, 128),
        routes.T,
        route_weights.T,
        w_gate,
        w_up,
        w_down,
        shared_gate,
        shared_up,
        shared_down,
    )
    return pl.pallas_call(
        functools.partial(kernel, kv_group=kv_group, order=order, near=near, nx=nx),
        out_shape=jax.ShapeDtypeStruct((tok, dc), BF),
        in_specs=[pl.BlockSpec(memory_space=pl.ANY)] * 15,
        out_specs=pl.BlockSpec(memory_space=vm),
        scratch_shapes=[
            *[vm(a.shape, a.dtype) for a in inputs],
            dma((len(inputs),)),
            vm((n_tp, w_out.shape[0], dc), BF),
            vm((n_tp, rows, dc), BF),
            vm((4, WINDOW, 2 * HD), BF),
            vm((n_tp, HD, tok), BF),
            vm((tok, d_model), BF),
            vm((exp_dev, n_rows, d_model), BF),
            vm(((1 + 2 * max(near)) * n_sp, exp_dev, slots, dc), BF),
            vm((n_tp * fh, tok), BF),
            vm((exp_dev, n_tp * fh, n_rows), BF),
            vm((exp_dev, n_rows, dc), BF),
            vm((n_sp, exp_dev, slots, dc), BF),
            vm((experts * slots, tok), BF),
            vm((tok, experts * slots), BF),
            vm((experts, tok), F32),
            vm((exp_dev + 1, 2 * fh, d_model), BF),
            vm((exp_dev + 1, dc, n_tp * fh), BF),
            vm((tok, dc), BF),
            vm((tok, dc), F32),
            dma((2,)),
            dma((max(nx - 1, 1),)),
            dma((max(nx - 1, 1),)),
            dma((2,)),
            dma((4,)),
            dma((4,)),
            dma(()),
            dma((n_tp,)),
            dma(()),
            dma((n_chunk, 1 + 2 * max(near))),
            dma(()),
            dma(()),
            dma(()),
            dma((n_tp,)),
            dma((n_chunk,)),
            dma((n_chunk, n_tp)),
            dma(()),
            dma((n_tp,)),
            dma((n_chunk,)),
            dma((n_chunk, n_tp)),
        ],
        compiler_params=pltpu.CompilerParams(
            collective_id=0, has_side_effects=True, vmem_limit_bytes=60 * 1024 * 1024
        ),
    )(*inputs)


def solution(mesh, kv_group=4, order=Z_ORDER, near=NEAR, nx=NX):
    placed = (
        P("sp", "tp"),
        P("sp", None),
        P("sp", None),
        P("tp"),
        P("tp", None),
        P(("sp", "tp"), None),
        P(),
        P("sp", None),
        P("sp", None),
        P("sp", "tp", None),
        P("sp", "tp", None),
        P("sp", None, "tp"),
        P("tp", None),
        P("tp", None),
        P(None, "tp"),
    )
    return jax.shard_map(
        functools.partial(local, kv_group=kv_group, order=order, near=near, nx=nx),
        mesh=mesh,
        in_specs=placed,
        out_specs=P("sp", "tp"),
        check_vma=False,
    )
```
